32 devices in a mesh: sp: 8 (over z, x), tp: 4 (over y, core).
Axes of the slice: x: 2, y: 2, z: 4, core: 2. Of those that a mesh axis runs over, the one named last changes fastest.
Arguments:
- queries: bfloat16 [2048, 2048], P('sp', 'tp'), may hold values from -100 to 100
- key_columns: bfloat16 [1024, 2048], P('tp', 'sp'), may hold values from -24 to 24
- value_columns: bfloat16 [1024, 2048], P('tp', 'sp'), may hold values from -24 to 24
- sink_logits: float32 [32], P('tp'), may hold values from 3 to 7
- out_weight: bfloat16 [2048, 2048], P('tp'), may hold values from -0.1875 to 0.1875
- stream_in: bfloat16 [2048, 2048], P('sp'), may hold values from -3 to 3
- norm_gain: float32 [2048], replicated, may hold values from 0.1 to 1.9
- expert_ids: int32 [2048, 2], P('sp'), may hold values from 0 to 7, all different within a row; in each aligned block of 256 rows (0 to 255, 256 to 511, ...) at most 128 rows name the same one
- route_weights: float32 [2048, 2], P('sp'), may hold values from 0.1 to 0.7
- gate_weight: bfloat16 [8, 2048, 4096], P('sp', None, 'tp'), may hold values from -0.125 to 0.125
- up_weight: bfloat16 [8, 2048, 4096], P('sp', None, 'tp'), may hold values from -0.125 to 0.125
- down_weight: bfloat16 [8, 4096, 2048], P('sp', 'tp'), may hold values from -0.125 to 0.125
Outputs:
- layer_out: bfloat16 [2048, 2048], P('sp', 'tp')
The draws below stay inside these ranges and needn't reach their ends.
Inputs may be any that keep to these rules, and one draw needn't show every extreme that they name: `expert_ids`: each row names 2 different experts. In each aligned block of 256 tokens no expert is named by more than 128 rows, and in some blocks one expert is named by exactly 128 rows.
All inputs are finite; a program needn't handle non-finite values.
Results may differ from the reference program's by a relative error of at most 0.02.
Values may be sent and summed in bfloat16 or wider, within the bound.
A program may use at most 64 MiB of HBM per device.

```python
import math
import jax
import jax.numpy as jnp
import numpy as np
from jax import lax

D = 2048
QH = 32
KVH = 16
HD = 64
FFE = 4096
WINDOW = 128
TOP = 2
T_SP = 256
TOKENS = 2048
EXPERTS = 8
CAP = 128
N_SP = 8
N_TP = 4


def draw_queries(key, part):
    drawn = jnp.clip(jax.random.normal(jax.random.fold_in(key, 1), (TOKENS, QH * HD), jnp.float32), -6.0, 6.0)
    return drawn.astype(jnp.bfloat16)


def draw_key_columns(key, part):
    drawn = jnp.clip(jax.random.normal(jax.random.fold_in(key, 2), (KVH * HD, TOKENS), jnp.float32), -6.0, 6.0)
    return drawn.astype(jnp.bfloat16)


def strengthened(drawn, stream_key, source, target, shards_of, factor):
    def block_of(dim):
        return (jnp.arange(drawn.shape[dim]) // (drawn.shape[dim] // shards_of)).reshape((-1,) + (1,) * (drawn.ndim - 1 - dim))

    first = jax.random.permutation(stream_key, shards_of)[block_of(target)]
    second = (block_of(target) + shards_of // 2) % shards_of
    return jnp.where((block_of(source) == first) | (block_of(source) == second), factor * drawn, drawn)


def shard_levels(stream_key, dims, cuts, smallest, largest):
    def one(dim, shards_of):
        heights = jax.random.uniform(jax.random.fold_in(jax.random.fold_in(stream_key, 6), dim), (shards_of,), jnp.float32, smallest / len(cuts), largest / len(cuts))
        return jnp.repeat(jnp.exp(heights), dims[dim] // shards_of).reshape((-1,) + (1,) * (len(dims) - dim - 1))

    gain = one(*cuts[0])
    for cut in cuts[1:]:
        gain = gain * one(*cut)
    return gain


def routed_block(key, own, number, rows, amount, top, bound, lean):
    order = jax.random.permutation(key, amount)
    heavy_load, usual = load_shares(amount, rows * top, bound, lean, True), load_shares(amount, rows * top, bound, lean, False)
    places = jnp.arange(amount)

    def named(tallies, turn):
        used = int((tallies > 0).sum())
        fixed = max(1, used // 4)
        moved = fixed + (places - fixed + turn * (used - fixed)) % max(1, amount - fixed)
        return jnp.zeros((amount,), jnp.int32).at[order[jnp.where(places < fixed, places, moved)]].set(jnp.asarray(tallies, jnp.int32))

    tallies = jnp.where(number % 4 == 0, named(heavy_load, number // 4), named(usual, number - number // 4 - 1))
    mixed = jax.random.permutation(jax.random.fold_in(own, 3), amount)
    donor, sink = mixed[0:amount // 2 * 2:2], mixed[1:amount // 2 * 2:2]
    slack = jnp.minimum(tallies[donor] - 1, bound - tallies[sink]) // 2
    slack = jnp.where((donor == order[0]) | (sink == order[0]) | (tallies[sink] == 0), 0, jnp.maximum(slack, 0))
    moved = jax.random.randint(jax.random.fold_in(own, 4), (amount // 2,), 0, 1 << 20) % (slack + 1)
    tallies = tallies.at[donor].add(-moved).at[sink].add(moved)
    items = jnp.searchsorted(jnp.cumsum(tallies), jnp.arange(rows * top), side="right").astype(jnp.int32)
    table = items.reshape(top, rows).T
    table = table[jax.random.permutation(jax.random.fold_in(own, 1), rows)]
    turn = jax.random.randint(jax.random.fold_in(own, 2), (rows, 1), 0, top)
    return jnp.take_along_axis(table, (jnp.arange(top)[None, :] + turn) % top, axis=1)


def load_shares(amount, total, most, skew, full):
    loads = [(1 << 20) // math.isqrt(rank ** skew) + 1 for rank in range(1, amount + 1)]
    largest = most if full else min(most, max(-(-total // amount), total * loads[0] // sum(loads)))
    least = 1 if total - largest >= amount - 1 else 0
    counts, spare = [largest] + [least] * (amount - 1), total - largest - least * (amount - 1)
    while spare > 0:
        movable = [i for i in range(1, amount) if counts[i] < largest] or [i for i in range(1, amount) if counts[i] < most]
        mass, remaining = sum([loads[i] for i in movable]), spare
        for i in movable:
            extra = min(most - counts[i], max(1, remaining * loads[i] // mass), spare)
            counts[i] = counts[i] + extra
            spare = spare - extra
    return np.array(counts)


def centred(own_key, dims, deviation, most, pieces=(), held_as=jnp.bfloat16):
    drawn = deviation * jax.random.normal(own_key, dims, jnp.float32)
    if pieces:
        drawn = drawn * shard_levels(own_key, dims, pieces, -0.22, 0.18)
    return jnp.clip(drawn, -most, most).astype(held_as)


def bell_draw_with(rng, dims, spread, most, cuts, heavy, kind=jnp.bfloat16):
    values = spread * jax.random.normal(rng, dims, jnp.float32)
    if cuts:
        values = values * shard_levels(rng, dims, cuts, -0.22, 0.18)
    return jnp.clip(strengthened(values, jax.random.fold_in(rng, 3), *heavy), -most, most).astype(kind)


def setup_inputs(seed: int = 0) -> dict:
    key_of = jax.random.split(jax.random.key(seed), 13)
    queries = draw_queries(jax.random.fold_in(key_of[12], 71), 0)
    key_columns = draw_key_columns(jax.random.fold_in(key_of[12], 71), 0)
    value_columns = centred(key_of[2], (KVH * HD, TOKENS), 4.0, 24.0, ((0, 4), (1, 8)))
    sink_logits = jnp.clip(3.0 + 4.0 * jax.random.uniform(key_of[3], (QH,), jnp.float32) ** shard_levels(key_of[3], (QH,), ((0, 4),), -0.2, 0.2), 3.0, 7.0)
    out_weight = bell_draw_with(key_of[4], (QH * HD, D), (QH * HD) ** -0.5, 0.1875, ((0, 4),), (0, 1, 4, 2.0))
    stream_in = centred(key_of[5], (TOKENS, D), 0.5, 3.0, ((0, 8),))
    norm_gain = jnp.clip(1.0 + 0.18 * jax.random.normal(key_of[6], (D,), jnp.float32), 0.1, 1.9)
    expert_ids_keys = jax.random.split(jax.random.fold_in(key_of[7], 1), TOKENS // T_SP)
    expert_ids_turns = jax.random.permutation(jax.random.fold_in(key_of[7], 3), TOKENS // T_SP)
    expert_ids = jax.vmap(lambda own, number: routed_block(jax.random.fold_in(key_of[7], 2), own, number, T_SP, EXPERTS, TOP, CAP, 1))(expert_ids_keys, expert_ids_turns).reshape((TOKENS, TOP))
    route_weights = jnp.clip(0.1 + 0.59999999 * jax.random.uniform(key_of[8], (TOKENS, TOP), jnp.float32) ** shard_levels(key_of[8], (TOKENS, TOP), ((0, 8),), -0.2, 0.2), 0.1, 0.7)
    gate_weight = centred(key_of[9], (EXPERTS, D, FFE), D ** -0.5, 0.125, ((0, 8), (2, 4)))
    up_weight = centred(key_of[10], (EXPERTS, D, FFE), D ** -0.5, 0.125, ((0, 8), (2, 4)))
    down_weight = bell_draw_with(key_of[11], (EXPERTS, FFE, D), FFE ** -0.5, 0.125, ((0, 8), (1, 4)), (1, 2, 4, 2.0))
    return {"queries": queries, "key_columns": key_columns, "value_columns": value_columns, "sink_logits": sink_logits, "out_weight": out_weight, "stream_in": stream_in, "norm_gain": norm_gain, "expert_ids": expert_ids, "route_weights": route_weights, "gate_weight": gate_weight, "up_weight": up_weight, "down_weight": down_weight}


EPSILON = 1e-06
MASKED = -1e+30

def rounded(number):
    return lax.optimization_barrier(number.astype(jnp.bfloat16)).astype(jnp.float32)

def rms_scale(residual, norm_gain):
    widened = residual.astype(jnp.float32)
    inverse_rms = lax.rsqrt(lax.optimization_barrier(jnp.mean(widened * widened, axis=-1, keepdims=True)) + EPSILON)
    return (widened * inverse_rms * norm_gain.astype(jnp.float32)).astype(jnp.bfloat16)

def attend(queries, key_columns, value_columns, sink_logits):
    per_group = QH // KVH
    blocks = TOKENS // WINDOW
    key_span = 3 * WINDOW
    padding = jnp.zeros((KVH * HD, WINDOW), jnp.bfloat16)
    key_padded = jnp.concatenate([padding, key_columns, padding], axis=1)
    value_padded = jnp.concatenate([padding, value_columns, padding], axis=1)
    query_blocks = queries.reshape(blocks, WINDOW, KVH, per_group, HD)
    sink_logit = sink_logits.astype(jnp.float32).reshape(KVH, per_group)[:, :, None]

    def one_block(block_index):
        offset = (block_index * WINDOW).astype(jnp.int32)
        query_block = lax.dynamic_index_in_dim(query_blocks, block_index, 0, keepdims=False).astype(jnp.float32)
        key_block = lax.dynamic_slice_in_dim(key_padded, offset, key_span, 1).reshape(KVH, HD, key_span).astype(jnp.float32)
        value_block = lax.dynamic_slice_in_dim(value_padded, offset, key_span, 1).reshape(KVH, HD, key_span).astype(jnp.float32)
        scores = jnp.einsum('qkgd,kdj->kgqj', query_block, key_block) / math.sqrt(HD)
        query_pos = offset + jnp.arange(WINDOW, dtype=jnp.int32)
        key_pos = offset - WINDOW + jnp.arange(key_span, dtype=jnp.int32)
        visible = (jnp.abs(query_pos[:, None] - key_pos[None, :]) <= WINDOW) & (key_pos >= 0)[None, :] & (key_pos < TOKENS)[None, :]
        scores = jnp.where(visible, scores, MASKED)
        row_top = jnp.maximum(lax.optimization_barrier(jnp.max(scores, axis=-1)), sink_logit)
        exponent = jnp.where(visible, jnp.exp(scores - row_top[..., None]), 0.0)
        denominator = lax.optimization_barrier(jnp.sum(exponent, axis=-1)) + jnp.exp(sink_logit - row_top)
        attn_weights = (exponent / denominator[..., None]).astype(jnp.bfloat16)
        head_mix = jnp.einsum('kgqj,kdj->qkgd', attn_weights.astype(jnp.float32), value_block)
        return head_mix.reshape(WINDOW, QH * HD).astype(jnp.bfloat16)
    return lax.map(one_block, jnp.arange(blocks, dtype=jnp.int32)).reshape(TOKENS, QH * HD)

def project_heads(head_out, out_weight):
    group_width = QH * HD // N_TP

    def add_group(carry, group_index):
        offset = (group_index * group_width).astype(jnp.int32)
        head_piece = lax.dynamic_slice_in_dim(head_out, offset, group_width, 1)
        weight_rows = lax.dynamic_slice_in_dim(out_weight, offset, group_width, 0)
        return (carry + rounded(jnp.dot(head_piece, weight_rows, preferred_element_type=jnp.float32)), None)
    summed, unused = lax.scan(add_group, jnp.zeros((TOKENS, D), jnp.float32), jnp.arange(N_TP, dtype=jnp.int32))
    return summed

def one_expert(operands):
    expert_rows_in, gate_matrix, up_matrix, down_matrix = operands
    gate_pre = jnp.dot(expert_rows_in, gate_matrix, preferred_element_type=jnp.float32)
    upward = jnp.dot(expert_rows_in, up_matrix, preferred_element_type=jnp.float32)
    hidden = (jax.nn.silu(gate_pre) * upward).astype(jnp.bfloat16)
    group_width = FFE // N_TP

    def add_group(carry, group_index):
        offset = (group_index * group_width).astype(jnp.int32)
        hidden_piece = lax.dynamic_slice_in_dim(hidden, offset, group_width, 1)
        down_rows = lax.dynamic_slice_in_dim(down_matrix, offset, group_width, 0)
        return (carry + rounded(jnp.dot(hidden_piece, down_rows, preferred_element_type=jnp.float32)), None)
    summed, unused = lax.scan(add_group, jnp.zeros((expert_rows_in.shape[0], D), jnp.float32), jnp.arange(N_TP, dtype=jnp.int32))
    return summed.astype(jnp.bfloat16)

def reference(queries, key_columns, value_columns, sink_logits, out_weight, stream_in, norm_gain, expert_ids, route_weights, gate_weight, up_weight, down_weight):
    head_out = attend(queries, key_columns, value_columns, sink_logits)
    attn_sum = project_heads(head_out, out_weight)
    residual = (stream_in.astype(jnp.float32) + rounded(attn_sum)).astype(jnp.bfloat16)
    normed = rms_scale(residual, norm_gain)
    route_ids = expert_ids.reshape(N_SP, T_SP * TOP)
    route_hits = (route_ids[..., None] == jnp.arange(EXPERTS, dtype=jnp.int32)).astype(jnp.int32)
    earlier = jnp.cumsum(route_hits, axis=1) - route_hits
    slot_index = lax.optimization_barrier(jnp.sum(earlier * route_hits, axis=2)).astype(jnp.int32)
    source = jnp.broadcast_to(jnp.arange(N_SP, dtype=jnp.int32)[:, None], route_ids.shape)
    position = source * CAP + slot_index
    route_rows = jnp.repeat(normed.reshape(N_SP, T_SP, 1, D), TOP, axis=2).reshape(N_SP, T_SP * TOP, D)
    buffer = jnp.zeros((EXPERTS, N_SP * CAP, D), jnp.bfloat16).at[route_ids, position].set(route_rows)
    expert_out = lax.map(one_expert, (buffer, gate_weight, up_weight, down_weight))
    picked = expert_out[route_ids, position].reshape(TOKENS, TOP, D).astype(jnp.float32)
    expert_sum = lax.optimization_barrier(jnp.sum(picked * route_weights[:, :, None], axis=1))
    return (residual.astype(jnp.float32) + expert_sum).astype(jnp.bfloat16)
```

```python
import functools
import math

import jax
import jax.numpy as jnp
from jax import lax
from jax.experimental import pallas as pl
from jax.experimental.pallas import tpu as pltpu
from jax.sharding import PartitionSpec as P

HD = 64
WINDOW = 128
CORES = 2
BLOCKS = 2
EPSILON = 1e-06
MASKED = -1e30
MESH = pl.DeviceIdType.MESH
F32 = jnp.float32
BF16 = jnp.bfloat16
scope = jax.named_scope


def iota(shape, dim):
    return lax.broadcasted_iota(jnp.int32, shape, dim)


def dot(a, b):
    return jnp.dot(a, b, preferred_element_type=F32)


def dot_t(a, b):
    return lax.dot_general(a, b, (((1,), (1,)), ((), ())), preferred_element_type=F32)


def as_row(column):
    size = column.shape[0]
    eye = iota((size, size), 0) == iota((size, size), 1)
    return jnp.sum(jnp.where(eye, column, 0.0), axis=0, keepdims=True)


def as_column(row):
    size = row.shape[1]
    eye = iota((size, size), 0) == iota((size, size), 1)
    return jnp.sum(jnp.where(eye, row, 0.0), axis=1, keepdims=True)


def diagonal(a):
    zero = jnp.zeros(a.shape, a.dtype)
    return jnp.concatenate(
        [jnp.concatenate([a, zero], axis=1), jnp.concatenate([zero, a], axis=1)], axis=0
    )


def send(src, dst, send_sem, recv_sem, device):
    pltpu.make_async_remote_copy(
        src_ref=src,
        dst_ref=dst,
        send_sem=send_sem,
        recv_sem=recv_sem,
        device_id=device,
        device_id_type=MESH,
    ).start()


def sent(ref, sem, device):
    pltpu.make_async_remote_copy(
        src_ref=ref, dst_ref=ref, send_sem=sem, recv_sem=sem,
        device_id=device, device_id_type=MESH,
    ).wait_send()


def landed(ref, sem, device):
    pltpu.make_async_remote_copy(
        src_ref=ref, dst_ref=ref, send_sem=sem, recv_sem=sem,
        device_id=device, device_id_type=MESH,
    ).wait_recv()


def layer(
    n, tp, cap,
    q_hbm, k_hbm, v_hbm, sink_hbm, gain_hbm, ids_hbm, rw_hbm,
    ow_hbm, stream_hbm, gate_hbm, up_hbm, down_hbm,
    out_hbm,
    q_ref, k_ref, v_ref, sink_ref, gain_ref, ids_ref, rw_ref,
    ow, stream, gate, up, down,
    halo, own_o, own_m, head, part, part_in, part_sum, part_y, squares,
    pick, mixer, rows_out, slots, scale_out, scale_in, xb, hid,
    po, po_in, chip_sum, sum_y, final, back, mixed, residual, out,
    load_sem, halo_send, halo_recv, ps_send, ps_recv, py_send, py_recv, sq_send, sq_recv,
    d_send, x_recv, sc_send, sc_recv, fc_send, fy_send, f2_send,
    po_send, po_recv, y_send, y_recv, r_send, r_recv, out_sem,
):
    s, t = lax.axis_index("sp"), lax.axis_index("tp")
    ny = tp // CORES
    y, c = t // CORES, lax.rem(t, CORES)
    other = 1 - c
    tok, width = residual.shape
    hidden = gate.shape[1]
    top = ids_ref.shape[0]
    kv_heads = k_ref.shape[0] // HD

    def at_sp(i):
        return (i, t)

    def at_tp(j):
        return (s, j)

    partner = at_tp(y * CORES + other)

    def pair(i):
        total, bit = 0, 1
        while bit < n:
            total = total + lax.rem(s // bit + i // bit, 2) * bit
            bit *= 2
        return total

    def peer_y(dy):
        return lax.rem(y + dy, ny)

    def from_y(dy):
        return lax.rem(y + ny - dy, ny)

    own_cols = pl.ds(pl.multiple_of(t * width, 128), width)
    loads = [
        pltpu.make_async_copy(src, dst, load_sem.at[i])
        for i, (src, dst) in enumerate((
            (k_hbm, k_ref), (v_hbm, v_ref), (q_hbm, q_ref), (ids_hbm, ids_ref),
            (sink_hbm, sink_ref), (rw_hbm, rw_ref), (gain_hbm, gain_ref),
            (ow_hbm, ow), (stream_hbm.at[:, own_cols], stream),
            (gate_hbm.at[0], gate), (up_hbm.at[0], up), (down_hbm.at[0], down),
        ))
    ]
    for load in loads[:7]:
        load.start()

    barrier = pltpu.get_barrier_semaphore()

    def greet_sp(i, _):
        pl.semaphore_signal(
            barrier, inc=1, device_id=at_sp(lax.rem(s + i, n)), device_id_type=MESH
        )
        return 0

    def greet_tp(j, _):
        pl.semaphore_signal(
            barrier, inc=1, device_id=at_tp(lax.rem(t + j, tp)), device_id_type=MESH
        )
        return 0

    lax.fori_loop(1, n, greet_sp, 0)
    lax.fori_loop(1, tp, greet_tp, 0)
    loads[0].wait()
    loads[1].wait()
    loads[3].wait()
    for load in loads[7:9]:
        load.start()
    with scope("barrier"):
        pl.semaphore_wait(barrier, n - 1 + tp - 1)

    right, left = at_sp(lax.rem(s + 1, n)), at_sp(lax.rem(s + n - 1, n))
    last = tok - WINDOW

    def send_right():
        @pl.when(s < n - 1)
        def _():
            for a, source in enumerate((k_ref, v_ref)):
                send(source.at[:, pl.ds(last, WINDOW)], halo.at[a, 0],
                     halo_send.at[a, 0], halo_recv.at[a, 0], right)

    def send_left():
        @pl.when(s > 0)
        def _():
            for a, source in enumerate((k_ref, v_ref)):
                send(source.at[:, pl.ds(0, WINDOW)], halo.at[a, 1],
                     halo_send.at[a, 1], halo_recv.at[a, 1], left)

    even = lax.rem(s, 2) == 0
    pl.when(even)(send_right)
    send_left()
    pl.when(jnp.logical_not(even))(send_right)
    for load in loads[9:]:
        load.start()

    @pl.when(s == 0)
    def _():
        for a in range(2):
            halo[a, 0] = jnp.zeros(halo.shape[2:], BF16)

    @pl.when(s == n - 1)
    def _():
        for a in range(2):
            halo[a, 1] = jnp.zeros(halo.shape[2:], BF16)

    loads[2].wait()
    loads[4].wait()
    square = (WINDOW, WINDOW)
    ahead = iota(square, 1) - iota(square, 0)
    low_lanes = iota(square, 1) < HD

    def query(b, g):
        rows = pl.ds(pl.multiple_of(b * WINDOW, WINDOW), WINDOW)
        return q_ref[rows, pl.ds(g * 2 * HD, 2 * HD)] * (1.0 / math.sqrt(HD))

    def mix_matrix(v):
        return jnp.concatenate([diagonal(v), diagonal(jnp.ones(v.shape, BF16))], axis=0)

    def sinks(g):
        return [sink_ref[0:1, 2 * g + h : 2 * g + h + 1] for h in range(2)]

    with scope("attn_own"):
        for g in range(kv_heads):
            feats = pl.ds(g * HD, HD)
            keys = diagonal(k_ref[feats, :])
            mixer_v = mix_matrix(v_ref[feats, :])
            for b in range(BLOCKS):
                scores = dot(query(b, g), keys)
                weights = []
                for h in range(2):
                    part_s = [
                        scores[:, h * tok + kb * WINDOW : h * tok + (kb + 1) * WINDOW]
                        for kb in range(BLOCKS)
                    ]
                    if b == 0:
                        part_s[1] = jnp.where(ahead <= 0, part_s[1], MASKED)
                    else:
                        part_s[0] = jnp.where(ahead >= 0, part_s[0], MASKED)
                    row_top = jnp.max(
                        jnp.maximum(part_s[0], part_s[1]), axis=1, keepdims=True
                    )
                    row_top = jnp.maximum(row_top, sinks(g)[h])
                    own_m[b, g, h] = jnp.broadcast_to(row_top, square)
                    weights += [jnp.exp(p - row_top).astype(BF16) for p in part_s]
                own_o[b, g] = dot_t(jnp.concatenate(weights, axis=1), mixer_v)

    with scope("routing"):
        lanes = iota((tok, 128), 1).astype(F32)
        ids = [as_column(ids_ref[k : k + 1, :].astype(F32)) for k in range(top)]
        hits = [(lanes == ids[k]).astype(F32) for k in range(top)]
        all_hits = functools.reduce(jnp.add, hits)
        before = (iota((tok, tok), 1) < iota((tok, tok), 0)).astype(BF16)
        earlier = dot(before, all_hits.astype(BF16))
        place = [
            jnp.sum(earlier * hits[k], axis=1, keepdims=True) + ids[k] * cap
            for k in range(top)
        ]
        place_row = [as_row(p) for p in place]
        loads[5].wait()
        share = [as_column(rw_ref[k : k + 1, :]) for k in range(top)]

        def picks(i, _):
            base = pair(i) * cap
            wanted = (iota((cap, tok), 0) + base).astype(F32)
            hit = functools.reduce(jnp.logical_or, [wanted == p for p in place_row])
            pick[pl.ds(pl.multiple_of(i * cap, cap), cap), :] = hit.astype(F32).astype(BF16)
            spot = (iota((tok, cap), 1) + base).astype(F32)
            weight = functools.reduce(
                jnp.add, [jnp.where(spot == p, w, 0.0) for p, w in zip(place, share)]
            )
            high = weight.astype(BF16)
            mixer[i] = jnp.concatenate([high, (weight - high.astype(F32)).astype(BF16)], axis=1)
            return 0

        lax.fori_loop(0, n, picks, 0)
    loads[6].wait()
    loads[7].wait()
    loads[8].wait()
    gain = gain_ref[:, own_cols]

    def attend(b):
        side = 1 - 2 * b
        edge = s + b * n
        inside = jnp.logical_and(edge > 0, edge < 2 * n - 1)

        @pl.when(inside)
        def _():
            for a in range(2):
                landed(halo.at[a, b], halo_recv.at[a, b], left)

        visible = (ahead * side >= 0) & (jnp.broadcast_to(inside.astype(jnp.int32), square) > 0)
        rows = pl.ds(pl.multiple_of(b * WINDOW, WINDOW), WINDOW)
        for g in range(kv_heads):
            feats = pl.ds(g * HD, HD)
            scores = dot(query(b, g), diagonal(halo[0, b, feats, :]))
            weights, gap, rest = [], [], []
            for h in range(2):
                piece = jnp.where(visible, scores[:, h * WINDOW : (h + 1) * WINDOW], MASKED)
                before_top = own_m[b, g, h]
                row_top = jnp.max(jnp.maximum(piece, before_top), axis=1, keepdims=True)
                weights.append(jnp.exp(piece - row_top).astype(BF16))
                gap.append(before_top - row_top)
                rest.append(jnp.broadcast_to(sinks(g)[h] - row_top, square))
            added = dot_t(
                jnp.concatenate(weights, axis=1), mix_matrix(halo[1, b, feats, :])
            )
            old = own_o[b, g]
            shrink = jnp.exp(jnp.where(low_lanes, gap[0], gap[1]))
            total = jnp.exp(jnp.where(low_lanes, rest[0], rest[1]))
            total = total + old[:, 2 * HD :] * shrink + added[:, 2 * HD :]
            value = old[:, : 2 * HD] * shrink + added[:, : 2 * HD]
            head[rows, pl.ds(g * 2 * HD, 2 * HD)] = (value / total).astype(BF16)

    def project(b, core):
        mine = head[pl.ds(pl.multiple_of(b * WINDOW, WINDOW), WINDOW), :]
        for yy in range(ny):
            start = pl.multiple_of((yy * CORES + core) * width, 128)
            part[b, core, yy] = dot(mine, ow[:, pl.ds(start, width)]).astype(BF16)

    def swap(b):
        project(b, other)
        send(part.at[b, other], part_in.at[b], ps_send.at[b], ps_recv.at[b], partner)
        project(b, c)

    def across(b):
        landed(part_in.at[b], ps_recv.at[b], partner)
        for dy in range(1, ny):
            yy = peer_y(dy)
            part_sum[b, dy] = (
                part[b, c, yy].astype(F32) + part_in[b, yy].astype(F32)
            ).astype(BF16)
            send(part_sum.at[b, dy], part_y.at[b, dy], py_send.at[b, dy], py_recv.at[b, dy],
                 at_tp(yy * CORES + c))

    def settle(b):
        attn = part[b, c, y].astype(F32) + part_in[b, y].astype(F32)
        for dy in range(1, ny):
            landed(part_y.at[b, dy], py_recv.at[b, dy], at_tp(from_y(dy) * CORES + c))
            attn = attn + part_y[b, dy].astype(F32)
        rows = pl.ds(pl.multiple_of(b * WINDOW, WINDOW), WINDOW)
        res = (stream[rows, :].astype(F32) + attn.astype(BF16).astype(F32)).astype(BF16)
        residual[rows, :] = res
        res = res.astype(F32)
        rows_out[rows, :] = (res * gain).astype(BF16)
        squares[0, :, rows] = jnp.broadcast_to(
            as_row(jnp.sum(res * res, axis=1, keepdims=True)), (8, WINDOW)
        )

    first = 1 - lax.rem(s, 2)
    second = 1 - first
    with scope("attend0"):
        attend(first)
    with scope("swap0"):
        swap(first)
    with scope("attend1"):
        attend(second)
    with scope("across0"):
        across(first)
    with scope("swap1"):
        swap(second)
    with scope("across1"):
        across(second)
    with scope("settle0"):
        settle(first)
    with scope("settle1"):
        settle(second)
    for dt in range(1, tp):
        send(squares.at[0], squares.at[dt], sq_send.at[dt], sq_recv.at[dt],
             at_tp(lax.rem(t + dt, tp)))

    def lane(k):
        return jnp.where(k < 2, k, jnp.where(k < 2 + n // 2, k - 2 + n // 2, k - n // 2))

    def rows_of(i):
        chosen = pick[pl.ds(pl.multiple_of(i * cap, cap), cap), :]
        return dot(chosen, rows_out[...]).astype(BF16)

    def forward(k):
        i = lane(k)

        @pl.when(i > 0)
        def _():
            landed(xb.at[t, i], x_recv.at[t, i], right)

        for dy in range(1, ny):
            send(xb.at[t, i], xb.at[t, i], fy_send.at[dy, i], x_recv.at[t, i],
                 at_tp(peer_y(dy) * CORES + c))
        send(xb.at[t, i], xb.at[t, i], fc_send.at[i], x_recv.at[t, i], partner)

    def dispatch(k, _):
        i = lane(k)
        slots[i] = rows_of(i)
        send(slots.at[i], xb.at[t, i], d_send.at[i], x_recv.at[t, i], at_sp(pair(i)))
        return 0

    with scope("dispatch"):
        xb[t, 0] = rows_of(0)
        forward(0)
        lax.fori_loop(1, n, dispatch, 0)

    with scope("scales"):
        square_sum = squares[0]
        for dt in range(1, tp):
            landed(squares.at[dt], sq_recv.at[dt], at_tp(lax.rem(t + tp - dt, tp)))
            square_sum = square_sum + squares[dt]
        inverse = lax.rsqrt(square_sum / (tp * width) + EPSILON)
        high = inverse.astype(BF16).astype(F32)
        middle = (inverse - high).astype(BF16).astype(F32)
        low = inverse - high - middle
        level = iota(inverse.shape, 0)
        pieces = jnp.where(
            level == 0, high, jnp.where(level == 1, middle, jnp.where(level == 2, low, 0.0))
        ).astype(BF16)
        scales = jnp.sum(dot_t(pieces, pick[...]), axis=0, keepdims=True)
        for i in range(n):
            piece = jnp.broadcast_to(scales[:, i * cap : (i + 1) * cap], (8, cap))
            if i == 0:
                scale_in[0] = piece
            else:
                scale_out[i] = piece
                send(scale_out.at[i], scale_in.at[i], sc_send.at[i], sc_recv.at[i],
                     at_sp(pair(i)))

    with scope("weights"):
        for load in loads[9:]:
            load.wait()

    def turn(j):
        return jnp.where(
            j < n // 2, j + n // 2, jnp.where(j < n - 2, j + 2 - n // 2, n - 1 - j)
        )

    def relay(k):
        i = lane(k)
        for dy in range(1, ny):
            j = from_y(dy) * CORES + c
            landed(xb.at[j, i], x_recv.at[j, i], at_tp(j))
            send(xb.at[j, i], xb.at[j, i], f2_send.at[dy, i], x_recv.at[j, i], partner)

    tile = min(hidden, 256)

    def expert(k):
        i = turn(k)
        for yy in range(ny):
            j = yy * CORES + other
            landed(xb.at[j, i], x_recv.at[j, i], partner)

        @pl.when(i > 0)
        def _():
            landed(scale_in.at[i], sc_recv.at[i], right)

        scale = as_column(scale_in[i, 0:1, :])
        rows = jnp.concatenate([xb[j, i] for j in range(tp)], axis=1)
        for f in range(hidden // tile):
            cols = pl.ds(f * tile, tile)
            gate_pre = dot(rows, gate[:, cols]) * scale
            upward = dot(rows, up[:, cols]) * scale
            hid[:, cols] = (gate_pre / (1.0 + jnp.exp(-gate_pre)) * upward).astype(BF16)
        for j in range(tp):
            po[i, j % CORES, j // CORES] = dot(
                hid[...], down[:, j * width : (j + 1) * width]
            ).astype(BF16)
        send(po.at[i, other], po_in.at[i], po_send.at[i], po_recv.at[i], partner)

    def chip_add(k):
        i = turn(k)
        landed(po_in.at[i], po_recv.at[i], partner)
        for dy in range(1, ny):
            yy = peer_y(dy)
            chip_sum[dy, i] = (po[i, c, yy].astype(F32) + po_in[i, yy].astype(F32)).astype(BF16)
            send(chip_sum.at[dy, i], sum_y.at[dy, i], y_send.at[dy, i], y_recv.at[dy, i],
                 at_tp(yy * CORES + c))

    def whole(i):
        total = po[i, c, y].astype(F32) + po_in[i, y].astype(F32)
        for dy in range(1, ny):
            landed(sum_y.at[dy, i], y_recv.at[dy, i], at_tp(from_y(dy) * CORES + c))
            total = total + sum_y[dy, i].astype(F32)
        return total.astype(BF16)

    def finish(k):
        i = turn(k)
        final[i] = whole(i)
        send(final.at[i], back.at[i], r_send.at[i], r_recv.at[i], at_sp(pair(i)))

    stages = (
        (0, n, forward), (5, n, chip_add), (1, n, relay), (4, n, expert), (6, n - 1, finish),
    )

    def step(k, _):
        for lag, count, stage in stages:
            first_step = max(lag, 1)

            @pl.when((k >= first_step) & (k - lag < count))
            def _(stage=stage, lag=lag):
                with scope(stage.__name__):
                    stage(k - lag)
        return 0

    lax.fori_loop(1, n + 5, step, 0)

    def blend(i):
        rows = back[i]
        return dot(mixer[i], jnp.concatenate([rows, rows], axis=0))

    def returned(i, _):
        landed(back.at[i], r_recv.at[i], right)
        mixed[...] += blend(i)
        return 0

    with scope("returned"):
        mixed[...] = residual[...].astype(F32)
        lax.fori_loop(2, n, returned, 0)

    with scope("drain"):
        @pl.when(s < n - 1)
        def _():
            for a in range(2):
                sent(halo.at[a, 0], halo_send.at[a, 0], right)

        @pl.when(s > 0)
        def _():
            for a in range(2):
                sent(halo.at[a, 1], halo_send.at[a, 1], left)

        for b in range(BLOCKS):
            sent(part_in.at[b], ps_send.at[b], partner)
            for dy in range(1, ny):
                sent(part_sum.at[b, dy], py_send.at[b, dy], partner)
        for dt in range(1, tp):
            sent(squares.at[0], sq_send.at[dt], partner)

        def drain(i, _):
            @pl.when(i > 0)
            def _():
                sent(slots.at[i], d_send.at[i], right)
                sent(scale_out.at[i], sc_send.at[i], right)

            @pl.when(i > 1)
            def _():
                sent(final.at[i], r_send.at[i], right)

            sent(final.at[i], fc_send.at[i], partner)
            sent(po_in.at[i], po_send.at[i], partner)
            for dy in range(1, ny):
                sent(final.at[i], fy_send.at[dy, i], partner)
                sent(final.at[i], f2_send.at[dy, i], partner)
            return 0

        lax.fori_loop(0, n, drain, 0)

    with scope("own"):
        back[0] = whole(0)
        mixed[...] += blend(0)

    with scope("near"):
        landed(back.at[1], r_recv.at[1], right)
        out[...] = (mixed[...] + blend(1)).astype(BF16)
    put = pltpu.make_async_copy(out, out_hbm, out_sem)
    put.start()
    sent(final.at[1], r_send.at[1], right)

    def drain_y(i, _):
        for dy in range(1, ny):
            sent(final.at[i], y_send.at[dy, i], partner)
        return 0

    with scope("exit"):
        lax.fori_loop(0, n, drain_y, 0)
        put.wait()


def local(
    n, tp,
    queries, key_columns, value_columns, sink_logits, out_weight, stream_in, norm_gain,
    expert_ids, route_weights, gate_weight, up_weight, down_weight,
):
    tok, features = stream_in.shape
    ny = tp // CORES
    cap = 4 * tok // n
    width = features // tp
    hidden = gate_weight.shape[2]
    kv = key_columns.shape[0]
    top = expert_ids.shape[1]
    heads = sink_logits.shape[0]
    groups = kv // HD
    assert tok == BLOCKS * WINDOW and heads == 2 * groups
    dma = pltpu.SemaphoreType.DMA
    anywhere = pl.BlockSpec(memory_space=pl.ANY)
    scratch = [
        pltpu.VMEM(queries.shape, BF16),
        pltpu.VMEM(key_columns.shape, BF16),
        pltpu.VMEM(value_columns.shape, BF16),
        pltpu.VMEM((1, heads), F32),
        pltpu.VMEM((1, features), F32),
        pltpu.VMEM((top, tok), jnp.int32),
        pltpu.VMEM((top, tok), F32),
        pltpu.VMEM(out_weight.shape, BF16),
        pltpu.VMEM((tok, width), BF16),
        pltpu.VMEM(gate_weight.shape[1:], BF16),
        pltpu.VMEM(up_weight.shape[1:], BF16),
        pltpu.VMEM(down_weight.shape[1:], BF16),
        pltpu.VMEM((2, 2, kv, WINDOW), BF16),
        pltpu.VMEM((BLOCKS, groups, WINDOW, 4 * HD), F32),
        pltpu.VMEM((BLOCKS, groups, 2, WINDOW, WINDOW), F32),
        pltpu.VMEM(queries.shape, BF16),
        pltpu.VMEM((BLOCKS, CORES, ny, WINDOW, width), BF16),
        pltpu.VMEM((BLOCKS, ny, WINDOW, width), BF16),
        pltpu.VMEM((BLOCKS, ny, WINDOW, width), BF16),
        pltpu.VMEM((BLOCKS, ny, WINDOW, width), BF16),
        pltpu.VMEM((tp, 8, tok), F32),
        pltpu.VMEM((n * cap, tok), BF16),
        pltpu.VMEM((n, tok, 2 * cap), BF16),
        pltpu.VMEM((tok, width), BF16),
        pltpu.VMEM((n, cap, width), BF16),
        pltpu.VMEM((n, 8, cap), F32),
        pltpu.VMEM((n, 8, cap), F32),
        pltpu.VMEM((tp, n, cap, width), BF16),
        pltpu.VMEM((cap, hidden), BF16),
        pltpu.VMEM((n, CORES, ny, cap, width), BF16),
        pltpu.VMEM((n, ny, cap, width), BF16),
        pltpu.VMEM((ny, n, cap, width), BF16),
        pltpu.VMEM((ny, n, cap, width), BF16),
        pltpu.VMEM((n, cap, width), BF16),
        pltpu.VMEM((n, cap, width), BF16),
        pltpu.VMEM((tok, width), F32),
        pltpu.VMEM((tok, width), BF16),
        pltpu.VMEM((tok, width), BF16),
        dma((12,)),
        dma((2, 2)), dma((2, 2)),
        dma((BLOCKS,)), dma((BLOCKS,)),
        dma((BLOCKS, ny)), dma((BLOCKS, ny)),
        dma((tp,)), dma((tp,)),
        dma((n,)), dma((tp, n)), dma((n,)), dma((n,)),
        dma((n,)), dma((ny, n)), dma((ny, n)),
        dma((n,)), dma((n,)),
        dma((ny, n)), dma((ny, n)),
        dma((n,)), dma((n,)),
        dma,
    ]
    return pl.pallas_call(
        functools.partial(layer, n, tp, cap),
        out_shape=jax.ShapeDtypeStruct((tok, width), BF16),
        in_specs=[anywhere] * 12,
        out_specs=anywhere,
        scratch_shapes=scratch,
        compiler_params=pltpu.CompilerParams(
            collective_id=0, has_side_effects=True, vmem_limit_bytes=60 * 1024 * 1024
        ),
    )(
        queries, key_columns, value_columns, sink_logits[None, :], norm_gain[None, :],
        expert_ids.T, route_weights.T, out_weight, stream_in, gate_weight, up_weight,
        down_weight,
    )


def solution(mesh):
    placed = (
        P("sp", "tp"),
        P("tp", "sp"),
        P("tp", "sp"),
        P("tp"),
        P("tp", None),
        P("sp", None),
        P(),
        P("sp", None),
        P("sp", None),
        P("sp", None, "tp"),
        P("sp", None, "tp"),
        P("sp", "tp", None),
    )
    return jax.shard_map(
        functools.partial(local, mesh.shape["sp"], mesh.shape["tp"]),
        mesh=mesh, in_specs=placed, out_specs=P("sp", "tp"), check_vma=False,
    )
```

```python
import functools
import math

import jax
import jax.numpy as jnp
from jax import lax
from jax.experimental import pallas as pl
from jax.experimental.pallas import tpu as pltpu
from jax.sharding import PartitionSpec as P

HD = 64
WINDOW = 128
CORES = 2
CHIPS_X = 2
BLOCKS = 2
EPSILON = 1e-06
MASKED = -1e30
MESH = pl.DeviceIdType.MESH
F32 = jnp.float32
BF16 = jnp.bfloat16
scope = jax.named_scope


def iota(shape, dim):
    return lax.broadcasted_iota(jnp.int32, shape, dim)


def dot(a, b):
    return jnp.dot(a, b, preferred_element_type=F32)


def dot_t(a, b):
    return lax.dot_general(a, b, (((1,), (1,)), ((), ())), preferred_element_type=F32)


def as_row(column):
    size = column.shape[0]
    eye = iota((size, size), 0) == iota((size, size), 1)
    return jnp.sum(jnp.where(eye, column, 0.0), axis=0, keepdims=True)


def as_column(row):
    size = row.shape[1]
    eye = iota((size, size), 0) == iota((size, size), 1)
    return jnp.sum(jnp.where(eye, row, 0.0), axis=1, keepdims=True)


def diagonal(a):
    zero = jnp.zeros(a.shape, a.dtype)
    return jnp.concatenate(
        [jnp.concatenate([a, zero], axis=1), jnp.concatenate([zero, a], axis=1)], axis=0
    )


def send(src, dst, send_sem, recv_sem, device):
    pltpu.make_async_remote_copy(
        src_ref=src,
        dst_ref=dst,
        send_sem=send_sem,
        recv_sem=recv_sem,
        device_id=device,
        device_id_type=MESH,
    ).start()


def sent(ref, sem, device):
    pltpu.make_async_remote_copy(
        src_ref=ref, dst_ref=ref, send_sem=sem, recv_sem=sem,
        device_id=device, device_id_type=MESH,
    ).wait_send()


def landed(ref, sem, device):
    pltpu.make_async_remote_copy(
        src_ref=ref, dst_ref=ref, send_sem=sem, recv_sem=sem,
        device_id=device, device_id_type=MESH,
    ).wait_recv()


def choose(k, table):
    value = table[-1]
    for at in range(len(table) - 2, -1, -1):
        value = jnp.where(k == at, table[at], value)
    return value


ROLES = (
    (
        "F3 F5 F4 R5",
        "F7 F1 R4 E5",
        "R3 C5 R7 E4",
        "F2 R1 C4 E7",
        "E1 R2 X5 C7",
        "E3 F6 R0 X4",
        "E2 C3 E0 X7",
        "R6 C1 C2 E6",
        "X3 X1 B7 C6",
        "B3 C0 X2 B4",
        "X6 B1 B5 B2",
        "B6",
    ),
    (
        "R0 F4 F3 F1",
        "R4 F2 E4 R3",
        "R1 C4 E0 F6",
        "E3 F7 R2 E1",
        "C3 R6 E2 F5",
        "X4 C1 E6 R7",
        "X3 C6 R5 E7",
        "E5 C7 X6 C5",
        "C2 X1 B5 X7",
        "C0 X5 X2 B3",
        "B1 B6 B4 B7",
        "B2",
    ),
)
SENDS = ((4, 3, 7, 1, 6, 5, 2), (3, 5, 4, 2, 1, 6, 7))


def plan(n):
    if n == 8:
        steps = [[(step[0], int(step[1:])) for step in " ".join(role).split()] for role in ROLES]
        return SENDS, steps
    order = [("R", 0)] + [(op, i) for i in range(1, n) for op in "FR"]
    late = list(range(n - 1, -1, -1))
    order += [(op, i) for i in late for op in "EC"]
    order += [(op, i) for op in "XB" for i in late if i]
    return [list(range(1, n))] * 2, [order] * 2


def layer(
    n, tp, cap,
    q_hbm, k_hbm, v_hbm, sink_hbm, gain_hbm, ids_hbm, rw_hbm,
    ow_hbm, stream_hbm, gate_hbm, up_hbm, down_hbm,
    out_hbm,
    q_ref, k_ref, v_ref, sink_ref, gain_ref, ids_ref, rw_ref,
    ow, stream, gate, up, down,
    halo, own_o, own_m, head, part, part_in, part_sum, part_y, squares,
    pick, mixer, rows_out, slots, scale_out, scale_in, xb, hid,
    po, po_in, chip_sum, sum_y, final, back, mixed, residual, out,
    load_sem, halo_send, halo_recv, ps_send, ps_recv, py_send, py_recv, sq_send, sq_recv,
    d_send, x_recv, sc_send, sc_recv, fc_send, fy_send, f2_send,
    po_send, po_recv, y_send, y_recv, r_send, r_recv, out_sem,
):
    s, t = lax.axis_index("sp"), lax.axis_index("tp")
    ny = tp // CORES
    y, c = t // CORES, lax.rem(t, CORES)
    other = 1 - c
    tok, width = residual.shape
    hidden = gate.shape[1]
    top = ids_ref.shape[0]
    kv_heads = k_ref.shape[0] // HD

    def at_sp(i):
        return (i, t)

    def at_tp(j):
        return (s, j)

    partner = at_tp(y * CORES + other)

    def pair(i):
        total, bit = 0, 1
        while bit < n:
            total = total + lax.rem(s // bit + i // bit, 2) * bit
            bit *= 2
        return total

    def peer_y(dy):
        return lax.rem(y + dy, ny)

    def from_y(dy):
        return lax.rem(y + ny - dy, ny)

    own_cols = pl.ds(pl.multiple_of(t * width, 128), width)
    loads = [
        pltpu.make_async_copy(src, dst, load_sem.at[i])
        for i, (src, dst) in enumerate((
            (k_hbm, k_ref), (v_hbm, v_ref), (q_hbm, q_ref), (ids_hbm, ids_ref),
            (sink_hbm, sink_ref), (rw_hbm, rw_ref), (gain_hbm, gain_ref),
            (ow_hbm, ow), (stream_hbm.at[:, own_cols], stream),
            (gate_hbm.at[0], gate), (up_hbm.at[0], up), (down_hbm.at[0], down),
        ))
    ]
    for load in loads[:7]:
        load.start()

    barrier = pltpu.get_barrier_semaphore()

    def greet_sp(i, _):
        pl.semaphore_signal(
            barrier, inc=1, device_id=at_sp(lax.rem(s + i, n)), device_id_type=MESH
        )
        return 0

    def greet_tp(j, _):
        pl.semaphore_signal(
            barrier, inc=1, device_id=at_tp(lax.rem(t + j, tp)), device_id_type=MESH
        )
        return 0

    lax.fori_loop(1, n, greet_sp, 0)
    lax.fori_loop(1, tp, greet_tp, 0)
    loads[0].wait()
    loads[1].wait()
    loads[3].wait()
    for load in loads[7:9]:
        load.start()
    with scope("barrier"):
        pl.semaphore_wait(barrier, n - 1 + tp - 1)

    right, left = at_sp(lax.rem(s + 1, n)), at_sp(lax.rem(s + n - 1, n))
    last = tok - WINDOW

    def send_right():
        @pl.when(s < n - 1)
        def _():
            for a, source in enumerate((k_ref, v_ref)):
                send(source.at[:, pl.ds(last, WINDOW)], halo.at[0, a],
                     halo_send.at[0], halo_recv.at[0], right)

    def send_left():
        @pl.when(s > 0)
        def _():
            for a, source in enumerate((k_ref, v_ref)):
                send(source.at[:, pl.ds(0, WINDOW)], halo.at[1, a],
                     halo_send.at[1], halo_recv.at[1], left)

    even = lax.rem(s, 2) == 0
    odd = jnp.logical_not(even)
    pl.when(even)(send_right)
    pl.when(odd)(send_left)
    for load in loads[9:]:
        load.start()

    @pl.when(s == 0)
    def _():
        halo[0] = jnp.zeros(halo.shape[1:], BF16)

    @pl.when(s == n - 1)
    def _():
        halo[1] = jnp.zeros(halo.shape[1:], BF16)

    loads[2].wait()
    loads[4].wait()
    square = (WINDOW, WINDOW)
    ahead = iota(square, 1) - iota(square, 0)
    low_lanes = iota(square, 1) < HD

    def query(b, g):
        rows = pl.ds(pl.multiple_of(b * WINDOW, WINDOW), WINDOW)
        return q_ref[rows, pl.ds(g * 2 * HD, 2 * HD)] * (1.0 / math.sqrt(HD))

    def mix_matrix(v):
        return jnp.concatenate([diagonal(v), diagonal(jnp.ones(v.shape, BF16))], axis=0)

    def sinks(g):
        return [sink_ref[0:1, 2 * g + h : 2 * g + h + 1] for h in range(2)]

    with scope("attn_own"):
        for g in range(kv_heads):
            feats = pl.ds(g * HD, HD)
            keys = diagonal(k_ref[feats, :])
            mixer_v = mix_matrix(v_ref[feats, :])
            for b in range(BLOCKS):
                scores = dot(query(b, g), keys)
                weights = []
                for h in range(2):
                    part_s = [
                        scores[:, h * tok + kb * WINDOW : h * tok + (kb + 1) * WINDOW]
                        for kb in range(BLOCKS)
                    ]
                    if b == 0:
                        part_s[1] = jnp.where(ahead <= 0, part_s[1], MASKED)
                    else:
                        part_s[0] = jnp.where(ahead >= 0, part_s[0], MASKED)
                    row_top = jnp.max(
                        jnp.maximum(part_s[0], part_s[1]), axis=1, keepdims=True
                    )
                    row_top = jnp.maximum(row_top, sinks(g)[h])
                    own_m[b, g, h] = jnp.broadcast_to(row_top, square)
                    weights += [jnp.exp(p - row_top).astype(BF16) for p in part_s]
                own_o[b, g] = dot_t(jnp.concatenate(weights, axis=1), mixer_v)

    with scope("routing"):
        lanes = iota((tok, 128), 1).astype(F32)
        before = (iota((tok, tok), 1) < iota((tok, tok), 0)).astype(BF16)

        ids = [as_column(ids_ref[k : k + 1, :].astype(F32)) for k in range(top)]
        hits = [(lanes == ids[k]).astype(F32) for k in range(top)]
        earlier = dot(before, functools.reduce(jnp.add, hits).astype(BF16))
        place = [
            jnp.sum(earlier * hits[k], axis=1, keepdims=True) + ids[k] * cap
            for k in range(top)
        ]
        place_row = [as_row(p) for p in place]
        loads[5].wait()
        share = [as_column(rw_ref[k : k + 1, :]) for k in range(top)]

        def picks(i, _):
            base = pair(i) * cap
            wanted = (iota((cap, tok), 0) + base).astype(F32)
            hit = functools.reduce(jnp.logical_or, [wanted == p for p in place_row])
            pick[pl.ds(pl.multiple_of(i * cap, cap), cap), :] = hit.astype(F32).astype(BF16)
            spot = (iota((tok, cap), 1) + base).astype(F32)
            weight = functools.reduce(
                jnp.add, [jnp.where(spot == p, w, 0.0) for p, w in zip(place, share)]
            )
            high = weight.astype(BF16)
            mixer[i] = jnp.concatenate([high, (weight - high.astype(F32)).astype(BF16)], axis=1)
            return 0

        lax.fori_loop(0, n, picks, 0)
    pl.when(even)(send_left)
    pl.when(odd)(send_right)
    loads[6].wait()
    loads[7].wait()
    loads[8].wait()
    gain = gain_ref[:, own_cols]

    def attend(b):
        side = 1 - 2 * b
        edge = s + b * n
        inside = jnp.logical_and(edge > 0, edge < 2 * n - 1)

        @pl.when(inside)
        def _():
            landed(halo.at[b], halo_recv.at[b], left)

        visible = (ahead * side >= 0) & (jnp.broadcast_to(inside.astype(jnp.int32), square) > 0)
        rows = pl.ds(pl.multiple_of(b * WINDOW, WINDOW), WINDOW)
        for g in range(kv_heads):
            feats = pl.ds(g * HD, HD)
            scores = dot(query(b, g), diagonal(halo[b, 0, feats, :]))
            weights, gap, rest = [], [], []
            for h in range(2):
                piece = jnp.where(visible, scores[:, h * WINDOW : (h + 1) * WINDOW], MASKED)
                before_top = own_m[b, g, h]
                row_top = jnp.max(jnp.maximum(piece, before_top), axis=1, keepdims=True)
                weights.append(jnp.exp(piece - row_top).astype(BF16))
                gap.append(before_top - row_top)
                rest.append(jnp.broadcast_to(sinks(g)[h] - row_top, square))
            added = dot_t(
                jnp.concatenate(weights, axis=1), mix_matrix(halo[b, 1, feats, :])
            )
            old = own_o[b, g]
            shrink = jnp.exp(jnp.where(low_lanes, gap[0], gap[1]))
            total = jnp.exp(jnp.where(low_lanes, rest[0], rest[1]))
            total = total + old[:, 2 * HD :] * shrink + added[:, 2 * HD :]
            value = old[:, : 2 * HD] * shrink + added[:, : 2 * HD]
            head[rows, pl.ds(g * 2 * HD, 2 * HD)] = (value / total).astype(BF16)

    def project(b, core):
        mine = head[pl.ds(pl.multiple_of(b * WINDOW, WINDOW), WINDOW), :]
        for yy in range(ny):
            start = pl.multiple_of((yy * CORES + core) * width, 128)
            part[b, core, yy] = dot(mine, ow[:, pl.ds(start, width)]).astype(BF16)

    def swap(b):
        project(b, other)
        send(part.at[b, other], part_in.at[b], ps_send, ps_recv.at[b], partner)
        project(b, c)

    def across(b):
        landed(part_in.at[b], ps_recv.at[b], partner)
        for dy in range(1, ny):
            yy = peer_y(dy)
            part_sum[b, dy] = (
                part[b, c, yy].astype(F32) + part_in[b, yy].astype(F32)
            ).astype(BF16)
            send(part_sum.at[b, dy], part_y.at[b, dy], py_send, py_recv.at[b, dy - 1],
                 at_tp(yy * CORES + c))

    def settle(b):
        attn = part[b, c, y].astype(F32) + part_in[b, y].astype(F32)
        for dy in range(1, ny):
            landed(part_y.at[b, dy], py_recv.at[b, dy - 1], at_tp(from_y(dy) * CORES + c))
            attn = attn + part_y[b, dy].astype(F32)
        rows = pl.ds(pl.multiple_of(b * WINDOW, WINDOW), WINDOW)
        res = (stream[rows, :].astype(F32) + attn.astype(BF16).astype(F32)).astype(BF16)
        residual[rows, :] = res
        res = res.astype(F32)
        rows_out[rows, :] = (res * gain).astype(BF16)
        squares[0, :, rows] = jnp.broadcast_to(
            as_row(jnp.sum(res * res, axis=1, keepdims=True)), (8, WINDOW)
        )

    first = 1 - lax.rem(s, 2)
    second = 1 - first
    with scope("attend0"):
        attend(first)
    with scope("swap0"):
        swap(first)
    with scope("attend1"):
        attend(second)
    with scope("across0"):
        across(first)
    with scope("swap1"):
        swap(second)
    with scope("across1"):
        across(second)
    with scope("settle0"):
        settle(first)
    with scope("settle1"):
        settle(second)
    for dt in range(1, tp):
        send(squares.at[0], squares.at[dt], sq_send, sq_recv.at[dt - 1],
             at_tp(lax.rem(t + dt, tp)))

    sends, steps = plan(n)
    place_z = s // CHIPS_X
    outer = (place_z == 0) | (place_z == n // CHIPS_X - 1)

    def by_role(k, tables):
        return jnp.where(outer, choose(k, tables[1]), choose(k, tables[0]))


    def chosen(i, source):
        rows = pick[pl.ds(pl.multiple_of(i * cap, cap), cap), :]
        return dot(rows, source[...]).astype(BF16)

    def forward(i):
        @pl.when(i > 0)
        def _():
            landed(xb.at[t, i], x_recv.at[t, i], right)

        for dy in range(1, ny):
            send(xb.at[t, i], xb.at[t, i], fy_send, x_recv.at[t, i],
                 at_tp(peer_y(dy) * CORES + c))
        send(xb.at[t, i], xb.at[t, i], fc_send, x_recv.at[t, i], partner)

    def dispatch(k, _):
        i = by_role(k, sends)
        slots[i] = chosen(i, rows_out)
        send(slots.at[i], xb.at[t, i], d_send, x_recv.at[t, i], at_sp(pair(i)))
        return 0

    with scope("dispatch"):
        xb[t, 0] = chosen(0, rows_out)
        forward(0)
        dispatch(0, 0)

    with scope("scales"):
        square_sum = squares[0]
        for dt in range(1, tp):
            landed(squares.at[dt], sq_recv.at[dt - 1], at_tp(lax.rem(t + tp - dt, tp)))
            square_sum = square_sum + squares[dt]
        inverse = lax.rsqrt(square_sum / (tp * width) + EPSILON)
        high = inverse.astype(BF16).astype(F32)
        middle = (inverse - high).astype(BF16).astype(F32)
        low = inverse - high - middle
        level = iota(inverse.shape, 0)
        pieces = jnp.where(
            level == 0, high, jnp.where(level == 1, middle, jnp.where(level == 2, low, 0.0))
        ).astype(BF16)
        scales = jnp.sum(dot_t(pieces, pick[...]), axis=0, keepdims=True)
        for i in range(n):
            piece = jnp.broadcast_to(scales[:, i * cap : (i + 1) * cap], (8, cap))
            if i == 0:
                scale_in[0] = piece
            else:
                scale_out[i] = piece
                send(scale_out.at[i], scale_in.at[i], sc_send, sc_recv.at[i],
                     at_sp(pair(i)))

    with scope("late"):
        lax.fori_loop(1, n - 1, dispatch, 0)

    with scope("weights"):
        for load in loads[9:]:
            load.wait()

    def relay(i):
        for dy in range(1, ny):
            j = from_y(dy) * CORES + c
            landed(xb.at[j, i], x_recv.at[j, i], at_tp(j))
            send(xb.at[j, i], xb.at[j, i], f2_send, x_recv.at[j, i], partner)

    tile = min(hidden, 256)

    def expert(i):
        for yy in range(ny):
            j = yy * CORES + other
            landed(xb.at[j, i], x_recv.at[j, i], partner)

        @pl.when(i > 0)
        def _():
            landed(scale_in.at[i], sc_recv.at[i], right)

        scale = as_column(scale_in[i, 0:1, :])
        rows = jnp.concatenate([xb[j, i] for j in range(tp)], axis=1)
        for f in range(hidden // tile):
            cols = pl.ds(f * tile, tile)
            gate_pre = dot(rows, gate[:, cols]) * scale
            upward = dot(rows, up[:, cols]) * scale
            hid[:, cols] = (gate_pre / (1.0 + jnp.exp(-gate_pre)) * upward).astype(BF16)
        for j in range(tp):
            po[i, j % CORES, j // CORES] = dot(
                hid[...], down[:, j * width : (j + 1) * width]
            ).astype(BF16)
        send(po.at[i, other], po_in.at[i], po_send, po_recv.at[i], partner)

    def chip_add(i):
        landed(po_in.at[i], po_recv.at[i], partner)
        for dy in range(1, ny):
            yy = peer_y(dy)
            chip_sum[dy, i] = (po[i, c, yy].astype(F32) + po_in[i, yy].astype(F32)).astype(BF16)
            send(chip_sum.at[dy, i], sum_y.at[dy, i], y_send, y_recv.at[dy - 1, i],
                 at_tp(yy * CORES + c))

    def whole(i):
        total = po[i, c, y].astype(F32) + po_in[i, y].astype(F32)
        for dy in range(1, ny):
            landed(sum_y.at[dy, i], y_recv.at[dy - 1, i], at_tp(from_y(dy) * CORES + c))
            total = total + sum_y[dy, i].astype(F32)
        return total.astype(BF16)

    def finish(i):
        final[i] = whole(i)
        send(final.at[i], back.at[i], r_send, r_recv.at[i], at_sp(pair(i)))

    def blend(i):
        rows = back[i]
        return dot(mixer[i], jnp.concatenate([rows, rows], axis=0))

    def returned(i):
        landed(back.at[i], r_recv.at[i], right)
        mixed[...] += blend(i)

    mixed[...] = residual[...].astype(F32)
    stages = dict(
        F=forward, R=relay, E=expert, C=chip_add, X=finish, B=returned
    )
    codes = [
        [list(stages).index(op) * n + i for op, i in order] for order in steps
    ]

    def step(k, _):
        code = by_role(k, codes)
        for at, (name, stage) in enumerate(stages.items()):
            @pl.when((code >= at * n) & (code < (at + 1) * n))
            def _(stage=stage, name=name, at=at):
                with scope(name):
                    stage(code - at * n)
        return 0

    lax.fori_loop(0, len(codes[0]), step, 0)

    with scope("drain"):
        @pl.when(s < n - 1)
        def _():
            sent(halo.at[0], halo_send.at[0], right)

        @pl.when(s > 0)
        def _():
            sent(halo.at[1], halo_send.at[1], left)

        others = pl.ds(1, ny - 1)
        sent(part_in, ps_send, partner)
        sent(part_sum.at[:, others], py_send, partner)
        sent(squares.at[pl.ds(1, tp - 1)], sq_send, partner)
        sent(slots.at[pl.ds(1, n - 1)], d_send, right)
        sent(scale_out.at[pl.ds(1, n - 1)], sc_send, right)
        sent(final, fc_send, partner)
        sent(po_in, po_send, partner)
        for sem in (fy_send, f2_send):
            sent(chip_sum.at[others], sem, partner)

    with scope("own"):
        back[0] = whole(0)
        out[...] = (mixed[...] + blend(0)).astype(BF16)
    put = pltpu.make_async_copy(out, out_hbm, out_sem)
    put.start()
    sent(chip_sum.at[others], y_send, partner)
    sent(final.at[pl.ds(1, n - 1)], r_send, right)
    put.wait()


def local(
    n, tp,
    queries, key_columns, value_columns, sink_logits, out_weight, stream_in, norm_gain,
    expert_ids, route_weights, gate_weight, up_weight, down_weight,
):
    tok, features = stream_in.shape
    ny = tp // CORES
    cap = 4 * tok // n
    width = features // tp
    hidden = gate_weight.shape[2]
    kv = key_columns.shape[0]
    top = expert_ids.shape[1]
    heads = sink_logits.shape[0]
    groups = kv // HD
    assert tok == BLOCKS * WINDOW and heads == 2 * groups
    dma = pltpu.SemaphoreType.DMA
    anywhere = pl.BlockSpec(memory_space=pl.ANY)
    scratch = [
        pltpu.VMEM(queries.shape, BF16),
        pltpu.VMEM(key_columns.shape, BF16),
        pltpu.VMEM(value_columns.shape, BF16),
        pltpu.VMEM((1, heads), F32),
        pltpu.VMEM((1, features), F32),
        pltpu.VMEM((top, tok), jnp.int32),
        pltpu.VMEM((top, tok), F32),
        pltpu.VMEM(out_weight.shape, BF16),
        pltpu.VMEM((tok, width), BF16),
        pltpu.VMEM(gate_weight.shape[1:], BF16),
        pltpu.VMEM(up_weight.shape[1:], BF16),
        pltpu.VMEM(down_weight.shape[1:], BF16),
        pltpu.VMEM((2, 2, kv, WINDOW), BF16),
        pltpu.VMEM((BLOCKS, groups, WINDOW, 4 * HD), F32),
        pltpu.VMEM((BLOCKS, groups, 2, WINDOW, WINDOW), F32),
        pltpu.VMEM(queries.shape, BF16),
        pltpu.VMEM((BLOCKS, CORES, ny, WINDOW, width), BF16),
        pltpu.VMEM((BLOCKS, ny, WINDOW, width), BF16),
        pltpu.VMEM((BLOCKS, ny, WINDOW, width), BF16),
        pltpu.VMEM((BLOCKS, ny, WINDOW, width), BF16),
        pltpu.VMEM((tp, 8, tok), F32),
        pltpu.VMEM((n * cap, tok), BF16),
        pltpu.VMEM((n, tok, 2 * cap), BF16),
        pltpu.VMEM((tok, width), BF16),
        pltpu.VMEM((n, cap, width), BF16),
        pltpu.VMEM((n, 8, cap), F32),
        pltpu.VMEM((n, 8, cap), F32),
        pltpu.VMEM((tp, n, cap, width), BF16),
        pltpu.VMEM((cap, hidden), BF16),
        pltpu.VMEM((n, CORES, ny, cap, width), BF16),
        pltpu.VMEM((n, ny, cap, width), BF16),
        pltpu.VMEM((ny, n, cap, width), BF16),
        pltpu.VMEM((ny, n, cap, width), BF16),
        pltpu.VMEM((n, cap, width), BF16),
        pltpu.VMEM((n, cap, width), BF16),
        pltpu.VMEM((tok, width), F32),
        pltpu.VMEM((tok, width), BF16),
        pltpu.VMEM((tok, width), BF16),
        dma((12,)),
        dma((2,)), dma((2,)),
        dma, dma((BLOCKS,)),
        dma, dma((BLOCKS, ny - 1)),
        dma, dma((tp - 1,)),
        dma, dma((tp, n)), dma, dma((n,)),
        dma, dma, dma,
        dma, dma((n,)),
        dma, dma((ny - 1, n)),
        dma, dma((n,)),
        dma,
    ]
    return pl.pallas_call(
        functools.partial(layer, n, tp, cap),
        out_shape=jax.ShapeDtypeStruct((tok, width), BF16),
        in_specs=[anywhere] * 12,
        out_specs=anywhere,
        scratch_shapes=scratch,
        compiler_params=pltpu.CompilerParams(
            collective_id=0, has_side_effects=True, vmem_limit_bytes=60 * 1024 * 1024
        ),
    )(
        queries, key_columns, value_columns, sink_logits[None, :], norm_gain[None, :],
        expert_ids.T, route_weights.T, out_weight, stream_in, gate_weight, up_weight,
        down_weight,
    )


def solution(mesh):
    placed = (
        P("sp", "tp"),
        P("tp", "sp"),
        P("tp", "sp"),
        P("tp"),
        P("tp", None),
        P("sp", None),
        P(),
        P("sp", None),
        P("sp", None),
        P("sp", None, "tp"),
        P("sp", None, "tp"),
        P("sp", "tp", None),
    )
    return jax.shard_map(
        functools.partial(local, mesh.shape["sp"], mesh.shape["tp"]),
        mesh=mesh, in_specs=placed, out_specs=P("sp", "tp"), check_vma=False,
    )
```

```python
import functools
import math

import jax
import jax.numpy as jnp
from jax import lax
from jax.experimental import pallas as pl
from jax.experimental.pallas import tpu as pltpu
from jax.sharding import PartitionSpec as P

HD = 64
WINDOW = 128
CORES = 2
CHIPS_X = 2
BLOCKS = 2
BASE = 256
DIGITS = 3
EARLY = (3, 3)
EPSILON = 1e-06
MASKED = -1e30
MESH = pl.DeviceIdType.MESH
F32 = jnp.float32
BF16 = jnp.bfloat16
scope = jax.named_scope


def iota(shape, dim):
    return lax.broadcasted_iota(jnp.int32, shape, dim)


def dot(a, b):
    return jnp.dot(a, b, preferred_element_type=F32)


def dot_t(a, b):
    return lax.dot_general(a, b, (((1,), (1,)), ((), ())), preferred_element_type=F32)


def as_row(column):
    size = column.shape[0]
    eye = iota((size, size), 0) == iota((size, size), 1)
    return jnp.sum(jnp.where(eye, column, 0.0), axis=0, keepdims=True)


def as_column(row):
    size = row.shape[1]
    eye = iota((size, size), 0) == iota((size, size), 1)
    return jnp.sum(jnp.where(eye, row, 0.0), axis=1, keepdims=True)


def diagonal(a):
    zero = jnp.zeros(a.shape, a.dtype)
    return jnp.concatenate(
        [jnp.concatenate([a, zero], axis=1), jnp.concatenate([zero, a], axis=1)], axis=0
    )


def send(src, dst, send_sem, recv_sem, device):
    pltpu.make_async_remote_copy(
        src_ref=src,
        dst_ref=dst,
        send_sem=send_sem,
        recv_sem=recv_sem,
        device_id=device,
        device_id_type=MESH,
    ).start()


def sent(ref, sem, device):
    pltpu.make_async_remote_copy(
        src_ref=ref, dst_ref=ref, send_sem=sem, recv_sem=sem,
        device_id=device, device_id_type=MESH,
    ).wait_send()


def landed(ref, sem, device):
    pltpu.make_async_remote_copy(
        src_ref=ref, dst_ref=ref, send_sem=sem, recv_sem=sem,
        device_id=device, device_id_type=MESH,
    ).wait_recv()


def choose(k, table):
    value = table[-1]
    for at in range(len(table) - 2, -1, -1):
        value = jnp.where(k == at, table[at], value)
    return value


ROLES = (
    (
        "F1 F4 F6 F3",
        "R4 F5 R1 E4",
        "C4 R3 E1 F2",
        "R6 E3 F7 E6",
        "R5 X4 C6 R0",
        "E5 C5 R2 X6",
        "C3 R7 E2 X5",
        "C1 E7 C2 E0",
        "X1 X3 C7 X2",
        "X7 B3 C0 B1",
        "B4 B5 B6 B2",
        "B7",
    ),
    (
        "F6 F1 R6 F3",
        "E6 R0 F2 R3",
        "R1 C6 E0 R2",
        "F7 E1 F4 E3",
        "C1 R7 X6 F5",
        "E7 R4 C7 E4",
        "C3 R5 E2 C4",
        "X7 E5 X3 C5",
        "C2 X4 X1 B6",
        "X5 B7 C0 X2",
        "B5 B3 B1 B2",
        "B4",
    ),
)
SENDS = ((1, 6, 2, 4, 7, 3, 5), (6, 1, 4, 3, 5, 2, 7))


def plan(n):
    if n == 8:
        steps = [[(step[0], int(step[1:])) for step in " ".join(role).split()] for role in ROLES]
        return SENDS, steps
    order = [("R", 0)] + [(op, i) for i in range(1, n) for op in "FR"]
    late = list(range(n - 1, -1, -1))
    order += [(op, i) for i in late for op in "EC"]
    order += [(op, i) for op in "XB" for i in late if i]
    return [list(range(1, n))] * 2, [order] * 2


def layer(
    n, tp, cap,
    q_hbm, k_hbm, v_hbm, sink_hbm, gain_hbm, ids_hbm, rw_hbm,
    ow_hbm, stream_hbm, gate_hbm, up_hbm, down_hbm,
    out_hbm,
    q_ref, k_ref, v_ref, sink_ref, gain_ref, ids_ref, rw_ref,
    ow, stream, gate, up, down,
    halo, own_o, own_m, head, part, part_in, part_sum, part_y, squares,
    pick, mixer, rows_out, slots, scale_out, scale_in, xb, hid,
    po, po_in, chip_sum, sum_y, final, back, mixed, residual, out,
    load_sem, halo_send, halo_recv, ps_send, ps_recv, py_send, py_recv, sq_send, sq_recv,
    d_send, x_recv, sc_send, sc_recv, fc_send, fy_send, f2_send,
    po_send, po_recv, y_send, y_recv, r_send, r_recv, out_sem,
):
    s, t = lax.axis_index("sp"), lax.axis_index("tp")
    ny = tp // CORES
    y, c = t // CORES, lax.rem(t, CORES)
    other = 1 - c
    tok, width = residual.shape
    hidden = gate.shape[1]
    top = ids_ref.shape[0]
    kv_heads = k_ref.shape[0] // HD

    def at_sp(i):
        return (i, t)

    def at_tp(j):
        return (s, j)

    partner = at_tp(y * CORES + other)

    def pair(i):
        total, bit = 0, 1
        while bit < n:
            total = total + lax.rem(s // bit + i // bit, 2) * bit
            bit *= 2
        return total

    def peer_y(dy):
        return lax.rem(y + dy, ny)

    def from_y(dy):
        return lax.rem(y + ny - dy, ny)

    own_cols = pl.ds(pl.multiple_of(t * width, 128), width)
    loads = [
        pltpu.make_async_copy(src, dst, load_sem.at[i])
        for i, (src, dst) in enumerate((
            (k_hbm, k_ref), (v_hbm, v_ref), (q_hbm, q_ref), (ids_hbm, ids_ref),
            (sink_hbm, sink_ref), (rw_hbm, rw_ref), (gain_hbm, gain_ref),
            (ow_hbm, ow), (stream_hbm.at[:, own_cols], stream),
            (gate_hbm.at[0], gate), (up_hbm.at[0], up), (down_hbm.at[0], down),
        ))
    ]
    for load in loads[:7]:
        load.start()

    barrier = pltpu.get_barrier_semaphore()

    def greet_sp(i, _):
        pl.semaphore_signal(
            barrier, inc=1, device_id=at_sp(lax.rem(s + i, n)), device_id_type=MESH
        )
        return 0

    def greet_tp(j, _):
        pl.semaphore_signal(
            barrier, inc=1, device_id=at_tp(lax.rem(t + j, tp)), device_id_type=MESH
        )
        return 0

    lax.fori_loop(1, n, greet_sp, 0)
    lax.fori_loop(1, tp, greet_tp, 0)
    loads[0].wait()
    loads[1].wait()
    loads[3].wait()
    for load in loads[7:9]:
        load.start()
    with scope("barrier"):
        pl.semaphore_wait(barrier, n - 1 + tp - 1)

    right, left = at_sp(lax.rem(s + 1, n)), at_sp(lax.rem(s + n - 1, n))
    last = tok - WINDOW

    def send_right():
        @pl.when(s < n - 1)
        def _():
            for a, source in enumerate((k_ref, v_ref)):
                send(source.at[:, pl.ds(last, WINDOW)], halo.at[0, a],
                     halo_send.at[0], halo_recv.at[0], right)

    def send_left():
        @pl.when(s > 0)
        def _():
            for a, source in enumerate((k_ref, v_ref)):
                send(source.at[:, pl.ds(0, WINDOW)], halo.at[1, a],
                     halo_send.at[1], halo_recv.at[1], left)

    even = lax.rem(s, 2) == 0
    odd = jnp.logical_not(even)
    pl.when(even)(send_right)
    pl.when(odd)(send_left)
    for load in loads[9:]:
        load.start()

    @pl.when(s == 0)
    def _():
        halo[0] = jnp.zeros(halo.shape[1:], BF16)

    @pl.when(s == n - 1)
    def _():
        halo[1] = jnp.zeros(halo.shape[1:], BF16)

    loads[2].wait()
    loads[4].wait()
    square = (WINDOW, WINDOW)
    ahead = iota(square, 1) - iota(square, 0)
    low_lanes = iota(square, 1) < HD

    def query(b, g):
        rows = pl.ds(pl.multiple_of(b * WINDOW, WINDOW), WINDOW)
        return q_ref[rows, pl.ds(g * 2 * HD, 2 * HD)] * (1.0 / math.sqrt(HD))

    def mix_matrix(v):
        return jnp.concatenate([diagonal(v), diagonal(jnp.ones(v.shape, BF16))], axis=0)

    def sinks(g):
        return [sink_ref[0:1, 2 * g + h : 2 * g + h + 1] for h in range(2)]

    with scope("attn_own"):
        for g in range(kv_heads):
            feats = pl.ds(g * HD, HD)
            keys = diagonal(k_ref[feats, :])
            mixer_v = mix_matrix(v_ref[feats, :])
            for b in range(BLOCKS):
                scores = dot(query(b, g), keys)
                weights = []
                for h in range(2):
                    part_s = [
                        scores[:, h * tok + kb * WINDOW : h * tok + (kb + 1) * WINDOW]
                        for kb in range(BLOCKS)
                    ]
                    if b == 0:
                        part_s[1] = jnp.where(ahead <= 0, part_s[1], MASKED)
                    else:
                        part_s[0] = jnp.where(ahead >= 0, part_s[0], MASKED)
                    row_top = jnp.max(
                        jnp.maximum(part_s[0], part_s[1]), axis=1, keepdims=True
                    )
                    row_top = jnp.maximum(row_top, sinks(g)[h])
                    own_m[b, g, h] = jnp.broadcast_to(row_top, square)
                    weights += [jnp.exp(p - row_top).astype(BF16) for p in part_s]
                own_o[b, g] = dot_t(jnp.concatenate(weights, axis=1), mixer_v)

    with scope("routing"):
        lanes = iota((tok, 128), 1).astype(F32)
        before = (iota((tok, tok), 1) < iota((tok, tok), 0)).astype(BF16)

        ids = [as_column(ids_ref[k : k + 1, :].astype(F32)) for k in range(top)]
        hits = [(lanes == ids[k]).astype(F32) for k in range(top)]
        earlier = dot(before, functools.reduce(jnp.add, hits).astype(BF16))
        place = [
            jnp.sum(earlier * hits[k], axis=1, keepdims=True) + ids[k] * cap
            for k in range(top)
        ]
        place_row = [as_row(p) for p in place]
        loads[5].wait()
        share = [as_column(rw_ref[k : k + 1, :]) for k in range(top)]

        def picks(i, _):
            base = pair(i) * cap
            wanted = (iota((cap, tok), 0) + base).astype(F32)
            hit = functools.reduce(jnp.logical_or, [wanted == p for p in place_row])
            pick[pl.ds(pl.multiple_of(i * cap, cap), cap), :] = hit.astype(F32).astype(BF16)
            spot = (iota((tok, cap), 1) + base).astype(F32)
            weight = functools.reduce(
                jnp.add, [jnp.where(spot == p, w, 0.0) for p, w in zip(place, share)]
            )
            high = weight.astype(BF16)
            mixer[i] = jnp.concatenate([high, (weight - high.astype(F32)).astype(BF16)], axis=1)
            return 0

        lax.fori_loop(0, n, picks, 0)
    pl.when(even)(send_left)
    pl.when(odd)(send_right)
    loads[6].wait()
    loads[7].wait()
    loads[8].wait()
    gain = gain_ref[:, own_cols]

    def attend(b):
        side = 1 - 2 * b
        edge = s + b * n
        inside = jnp.logical_and(edge > 0, edge < 2 * n - 1)

        @pl.when(inside)
        def _():
            landed(halo.at[b], halo_recv.at[b], left)

        visible = (ahead * side >= 0) & (jnp.broadcast_to(inside.astype(jnp.int32), square) > 0)
        rows = pl.ds(pl.multiple_of(b * WINDOW, WINDOW), WINDOW)
        for g in range(kv_heads):
            feats = pl.ds(g * HD, HD)
            scores = dot(query(b, g), diagonal(halo[b, 0, feats, :]))
            weights, gap, rest = [], [], []
            for h in range(2):
                piece = jnp.where(visible, scores[:, h * WINDOW : (h + 1) * WINDOW], MASKED)
                before_top = own_m[b, g, h]
                row_top = jnp.max(jnp.maximum(piece, before_top), axis=1, keepdims=True)
                weights.append(jnp.exp(piece - row_top).astype(BF16))
                gap.append(before_top - row_top)
                rest.append(jnp.broadcast_to(sinks(g)[h] - row_top, square))
            added = dot_t(
                jnp.concatenate(weights, axis=1), mix_matrix(halo[b, 1, feats, :])
            )
            old = own_o[b, g]
            shrink = jnp.exp(jnp.where(low_lanes, gap[0], gap[1]))
            total = jnp.exp(jnp.where(low_lanes, rest[0], rest[1]))
            total = total + old[:, 2 * HD :] * shrink + added[:, 2 * HD :]
            value = old[:, : 2 * HD] * shrink + added[:, : 2 * HD]
            head[rows, pl.ds(g * 2 * HD, 2 * HD)] = (value / total).astype(BF16)

    def project(b, core):
        mine = head[pl.ds(pl.multiple_of(b * WINDOW, WINDOW), WINDOW), :]
        for yy in range(ny):
            start = pl.multiple_of((yy * CORES + core) * width, 128)
            part[b, core, yy] = dot(mine, ow[:, pl.ds(start, width)]).astype(BF16)

    def swap(b):
        project(b, other)
        send(part.at[b, other], part_in.at[b], ps_send, ps_recv.at[b], partner)
        project(b, c)

    def across(b):
        landed(part_in.at[b], ps_recv.at[b], partner)
        for dy in range(1, ny):
            yy = peer_y(dy)
            part_sum[b, dy] = (
                part[b, c, yy].astype(F32) + part_in[b, yy].astype(F32)
            ).astype(BF16)
            send(part_sum.at[b, dy], part_y.at[b, dy], py_send, py_recv.at[b, dy - 1],
                 at_tp(yy * CORES + c))

    def settle(b):
        attn = part[b, c, y].astype(F32) + part_in[b, y].astype(F32)
        for dy in range(1, ny):
            landed(part_y.at[b, dy], py_recv.at[b, dy - 1], at_tp(from_y(dy) * CORES + c))
            attn = attn + part_y[b, dy].astype(F32)
        rows = pl.ds(pl.multiple_of(b * WINDOW, WINDOW), WINDOW)
        res = (stream[rows, :].astype(F32) + attn.astype(BF16).astype(F32)).astype(BF16)
        residual[rows, :] = res
        res = res.astype(F32)
        rows_out[rows, :] = (res * gain).astype(BF16)
        squares[0, :, rows] = jnp.broadcast_to(
            as_row(jnp.sum(res * res, axis=1, keepdims=True)), (8, WINDOW)
        )

    first = 1 - lax.rem(s, 2)
    second = 1 - first
    with scope("attend0"):
        attend(first)
    with scope("swap0"):
        swap(first)
    with scope("across0"):
        across(first)
    with scope("attend1"):
        attend(second)
    with scope("swap1"):
        swap(second)
    with scope("across1"):
        across(second)
    with scope("settle0"):
        settle(first)
    with scope("settle1"):
        settle(second)
    for dt in range(1, tp):
        send(squares.at[0], squares.at[dt], sq_send, sq_recv.at[dt - 1],
             at_tp(lax.rem(t + dt, tp)))

    sends, steps = plan(n)
    place_z = s // CHIPS_X
    outer = (place_z == 0) | (place_z == n // CHIPS_X - 1)

    def packed(tables):
        tables = [table + [0] * (-len(table) % DIGITS) for table in map(list, tables)]
        words = [
            [sum(d * BASE**p for p, d in enumerate(table[at : at + DIGITS]))
             for at in range(0, len(table), DIGITS)]
            for table in tables
        ]
        return [jnp.where(outer, b, a) for a, b in zip(*words)]

    def unpacked(k, words):
        word = choose(k // DIGITS, words)
        return choose(k % DIGITS, [word // BASE**p % BASE for p in range(DIGITS)])

    send_words = packed(sends)
    early = jnp.where(outer, EARLY[1], EARLY[0])


    def chosen(i, source):
        rows = pick[pl.ds(pl.multiple_of(i * cap, cap), cap), :]
        return dot(rows, source[...]).astype(BF16)

    def forward(i):
        @pl.when(i > 0)
        def _():
            landed(xb.at[t, i], x_recv.at[t, i], right)

        for dy in range(1, ny):
            send(xb.at[t, i], xb.at[t, i], fy_send, x_recv.at[t, i],
                 at_tp(peer_y(dy) * CORES + c))
        send(xb.at[t, i], xb.at[t, i], fc_send, x_recv.at[t, i], partner)

    def dispatch(k, _):
        i = unpacked(k, send_words)
        slots[i] = chosen(i, rows_out)
        send(slots.at[i], xb.at[t, i], d_send, x_recv.at[t, i], at_sp(pair(i)))
        return 0

    with scope("dispatch"):
        xb[t, 0] = chosen(0, rows_out)
        forward(0)
        lax.fori_loop(0, early, dispatch, 0)

    with scope("scales"):
        square_sum = squares[0]
        for dt in range(1, tp):
            landed(squares.at[dt], sq_recv.at[dt - 1], at_tp(lax.rem(t + tp - dt, tp)))
            square_sum = square_sum + squares[dt]
        inverse = lax.rsqrt(square_sum / (tp * width) + EPSILON)
        high = inverse.astype(BF16).astype(F32)
        middle = (inverse - high).astype(BF16).astype(F32)
        low = inverse - high - middle
        level = iota(inverse.shape, 0)
        pieces = jnp.where(
            level == 0, high, jnp.where(level == 1, middle, jnp.where(level == 2, low, 0.0))
        ).astype(BF16)
        scales = jnp.sum(dot_t(pieces, pick[...]), axis=0, keepdims=True)
        for i in range(n):
            piece = jnp.broadcast_to(scales[:, i * cap : (i + 1) * cap], (8, cap))
            if i == 0:
                scale_in[0] = piece
            else:
                scale_out[i] = piece
                send(scale_out.at[i], scale_in.at[i], sc_send, sc_recv.at[i],
                     at_sp(pair(i)))

    with scope("late"):
        lax.fori_loop(early, n - 1, dispatch, 0)

    with scope("weights"):
        for load in loads[9:]:
            load.wait()

    def relay(i):
        for dy in range(1, ny):
            j = from_y(dy) * CORES + c
            landed(xb.at[j, i], x_recv.at[j, i], at_tp(j))
            send(xb.at[j, i], xb.at[j, i], f2_send, x_recv.at[j, i], partner)

    tile = min(hidden, 256)

    def expert(i):
        for yy in range(ny):
            j = yy * CORES + other
            landed(xb.at[j, i], x_recv.at[j, i], partner)

        @pl.when(i > 0)
        def _():
            landed(scale_in.at[i], sc_recv.at[i], right)

        scale = as_column(scale_in[i, 0:1, :])
        rows = jnp.concatenate([xb[j, i] for j in range(tp)], axis=1)
        for f in range(hidden // tile):
            cols = pl.ds(f * tile, tile)
            gate_pre = dot(rows, gate[:, cols]) * scale
            upward = dot(rows, up[:, cols]) * scale
            hid[:, cols] = (gate_pre / (1.0 + jnp.exp(-gate_pre)) * upward).astype(BF16)
        activated = hid[...]

        def lower(core):
            for yy in range(ny):
                start = pl.multiple_of((yy * CORES + core) * width, 128)
                po[i, core, yy] = dot(activated, down[:, pl.ds(start, width)]).astype(BF16)

        lower(other)
        send(po.at[i, other], po_in.at[i], po_send, po_recv.at[i], partner)
        lower(c)

    def chip_add(i):
        landed(po_in.at[i], po_recv.at[i], partner)
        for dy in range(1, ny):
            yy = peer_y(dy)
            chip_sum[dy, i] = (po[i, c, yy].astype(F32) + po_in[i, yy].astype(F32)).astype(BF16)
            send(chip_sum.at[dy, i], sum_y.at[dy, i], y_send, y_recv.at[dy - 1, i],
                 at_tp(yy * CORES + c))

    def whole(i):
        total = po[i, c, y].astype(F32) + po_in[i, y].astype(F32)
        for dy in range(1, ny):
            landed(sum_y.at[dy, i], y_recv.at[dy - 1, i], at_tp(from_y(dy) * CORES + c))
            total = total + sum_y[dy, i].astype(F32)
        return total.astype(BF16)

    def finish(i):
        final[i] = whole(i)
        send(final.at[i], back.at[i], r_send, r_recv.at[i], at_sp(pair(i)))

    def blend(i):
        rows = back[i]
        return dot(mixer[i], jnp.concatenate([rows, rows], axis=0))

    def returned(i):
        landed(back.at[i], r_recv.at[i], right)
        mixed[...] += blend(i)

    mixed[...] = residual[...].astype(F32)
    stages = dict(
        F=forward, R=relay, E=expert, C=chip_add, X=finish, B=returned
    )
    codes = [
        [list(stages).index(op) * n + i for op, i in order] for order in steps
    ]

    code_words = packed(codes)

    def step(k, _):
        code = unpacked(k, code_words)
        for at, (name, stage) in enumerate(stages.items()):
            @pl.when((code >= at * n) & (code < (at + 1) * n))
            def _(stage=stage, name=name, at=at):
                with scope(name):
                    stage(code - at * n)
        return 0

    lax.fori_loop(0, len(codes[0]), step, 0)

    with scope("drain"):
        @pl.when(s < n - 1)
        def _():
            sent(halo.at[0], halo_send.at[0], right)

        @pl.when(s > 0)
        def _():
            sent(halo.at[1], halo_send.at[1], left)

        others = pl.ds(1, ny - 1)
        sent(part_in, ps_send, partner)
        sent(part_sum.at[:, others], py_send, partner)
        sent(squares.at[pl.ds(1, tp - 1)], sq_send, partner)
        sent(slots.at[pl.ds(1, n - 1)], d_send, right)
        sent(scale_out.at[pl.ds(1, n - 1)], sc_send, right)
        sent(final, fc_send, partner)
        sent(po_in, po_send, partner)
        for sem in (fy_send, f2_send):
            sent(chip_sum.at[others], sem, partner)

    with scope("own"):
        back[0] = whole(0)
        out[...] = (mixed[...] + blend(0)).astype(BF16)
    put = pltpu.make_async_copy(out, out_hbm, out_sem)
    put.start()
    sent(chip_sum.at[others], y_send, partner)
    sent(final.at[pl.ds(1, n - 1)], r_send, right)
    put.wait()


def local(
    n, tp,
    queries, key_columns, value_columns, sink_logits, out_weight, stream_in, norm_gain,
    expert_ids, route_weights, gate_weight, up_weight, down_weight,
):
    tok, features = stream_in.shape
    ny = tp // CORES
    cap = 4 * tok // n
    width = features // tp
    hidden = gate_weight.shape[2]
    kv = key_columns.shape[0]
    top = expert_ids.shape[1]
    heads = sink_logits.shape[0]
    groups = kv // HD
    assert tok == BLOCKS * WINDOW and heads == 2 * groups
    dma = pltpu.SemaphoreType.DMA
    anywhere = pl.BlockSpec(memory_space=pl.ANY)
    scratch = [
        pltpu.VMEM(queries.shape, BF16),
        pltpu.VMEM(key_columns.shape, BF16),
        pltpu.VMEM(value_columns.shape, BF16),
        pltpu.VMEM((1, heads), F32),
        pltpu.VMEM((1, features), F32),
        pltpu.VMEM((top, tok), jnp.int32),
        pltpu.VMEM((top, tok), F32),
        pltpu.VMEM(out_weight.shape, BF16),
        pltpu.VMEM((tok, width), BF16),
        pltpu.VMEM(gate_weight.shape[1:], BF16),
        pltpu.VMEM(up_weight.shape[1:], BF16),
        pltpu.VMEM(down_weight.shape[1:], BF16),
        pltpu.VMEM((2, 2, kv, WINDOW), BF16),
        pltpu.VMEM((BLOCKS, groups, WINDOW, 4 * HD), F32),
        pltpu.VMEM((BLOCKS, groups, 2, WINDOW, WINDOW), F32),
        pltpu.VMEM(queries.shape, BF16),
        pltpu.VMEM((BLOCKS, CORES, ny, WINDOW, width), BF16),
        pltpu.VMEM((BLOCKS, ny, WINDOW, width), BF16),
        pltpu.VMEM((BLOCKS, ny, WINDOW, width), BF16),
        pltpu.VMEM((BLOCKS, ny, WINDOW, width), BF16),
        pltpu.VMEM((tp, 8, tok), F32),
        pltpu.VMEM((n * cap, tok), BF16),
        pltpu.VMEM((n, tok, 2 * cap), BF16),
        pltpu.VMEM((tok, width), BF16),
        pltpu.VMEM((n, cap, width), BF16),
        pltpu.VMEM((n, 8, cap), F32),
        pltpu.VMEM((n, 8, cap), F32),
        pltpu.VMEM((tp, n, cap, width), BF16),
        pltpu.VMEM((cap, hidden), BF16),
        pltpu.VMEM((n, CORES, ny, cap, width), BF16),
        pltpu.VMEM((n, ny, cap, width), BF16),
        pltpu.VMEM((ny, n, cap, width), BF16),
        pltpu.VMEM((ny, n, cap, width), BF16),
        pltpu.VMEM((n, cap, width), BF16),
        pltpu.VMEM((n, cap, width), BF16),
        pltpu.VMEM((tok, width), F32),
        pltpu.VMEM((tok, width), BF16),
        pltpu.VMEM((tok, width), BF16),
        dma((12,)),
        dma((2,)), dma((2,)),
        dma, dma((BLOCKS,)),
        dma, dma((BLOCKS, ny - 1)),
        dma, dma((tp - 1,)),
        dma, dma((tp, n)), dma, dma((n,)),
        dma, dma, dma,
        dma, dma((n,)),
        dma, dma((ny - 1, n)),
        dma, dma((n,)),
        dma,
    ]
    return pl.pallas_call(
        functools.partial(layer, n, tp, cap),
        out_shape=jax.ShapeDtypeStruct((tok, width), BF16),
        in_specs=[anywhere] * 12,
        out_specs=anywhere,
        scratch_shapes=scratch,
        compiler_params=pltpu.CompilerParams(
            collective_id=0, has_side_effects=True, vmem_limit_bytes=60 * 1024 * 1024
        ),
    )(
        queries, key_columns, value_columns, sink_logits[None, :], norm_gain[None, :],
        expert_ids.T, route_weights.T, out_weight, stream_in, gate_weight, up_weight,
        down_weight,
    )


def solution(mesh):
    placed = (
        P("sp", "tp"),
        P("tp", "sp"),
        P("tp", "sp"),
        P("tp"),
        P("tp", None),
        P("sp", None),
        P(),
        P("sp", None),
        P("sp", None),
        P("sp", None, "tp"),
        P("sp", None, "tp"),
        P("sp", "tp", None),
    )
    return jax.shard_map(
        functools.partial(local, mesh.shape["sp"], mesh.shape["tp"]),
        mesh=mesh, in_specs=placed, out_specs=P("sp", "tp"), check_vma=False,
    )
```

```python
import functools
import math

import jax
import jax.numpy as jnp
from jax import lax
from jax.experimental import pallas as pl
from jax.experimental.pallas import tpu as pltpu
from jax.sharding import PartitionSpec as P

HD = 64
WINDOW = 128
CORES = 2
CHIPS_X = 2
BLOCKS = 2
BASE = 256
DIGITS = 3
EARLY = (3, 3)
EPSILON = 1e-06
MASKED = -1e30
MESH = pl.DeviceIdType.MESH
F32 = jnp.float32
BF16 = jnp.bfloat16
scope = jax.named_scope


def iota(shape, dim):
    return lax.broadcasted_iota(jnp.int32, shape, dim)


def dot(a, b):
    return jnp.dot(a, b, preferred_element_type=F32)


def dot_t(a, b):
    return lax.dot_general(a, b, (((1,), (1,)), ((), ())), preferred_element_type=F32)


def as_row(column):
    size = column.shape[0]
    eye = iota((size, size), 0) == iota((size, size), 1)
    return jnp.sum(jnp.where(eye, column, 0.0), axis=0, keepdims=True)


def as_column(row):
    size = row.shape[1]
    eye = iota((size, size), 0) == iota((size, size), 1)
    return jnp.sum(jnp.where(eye, row, 0.0), axis=1, keepdims=True)


def diagonal(a):
    zero = jnp.zeros(a.shape, a.dtype)
    return jnp.concatenate(
        [jnp.concatenate([a, zero], axis=1), jnp.concatenate([zero, a], axis=1)], axis=0
    )


def send(src, dst, send_sem, recv_sem, device):
    pltpu.make_async_remote_copy(
        src_ref=src,
        dst_ref=dst,
        send_sem=send_sem,
        recv_sem=recv_sem,
        device_id=device,
        device_id_type=MESH,
    ).start()


def sent(ref, sem, device):
    pltpu.make_async_remote_copy(
        src_ref=ref, dst_ref=ref, send_sem=sem, recv_sem=sem,
        device_id=device, device_id_type=MESH,
    ).wait_send()


def landed(ref, sem, device):
    pltpu.make_async_remote_copy(
        src_ref=ref, dst_ref=ref, send_sem=sem, recv_sem=sem,
        device_id=device, device_id_type=MESH,
    ).wait_recv()


def choose(k, table):
    value = table[-1]
    for at in range(len(table) - 2, -1, -1):
        value = jnp.where(k == at, table[at], value)
    return value


ROLES = (
    (
        "F1 F4 F6 F3",
        "R4 F5 R1 E4",
        "C4 R3 E1 F2",
        "R6 E3 F7 E6",
        "R5 X4 C6 E5",
        "C5 R0 R2 X6",
        "C3 R7 E2 X5",
        "C1 E7 C2 E0",
        "X1 X3 C7 X2",
        "X7 B3 C0 B1",
        "B4 B5 B6 B2",
        "B7",
    ),
    (
        "F6 F1 R6 F3",
        "E6 R0 F2 R3",
        "R1 C6 E0 R2",
        "F7 E1 F4 E3",
        "C1 R7 X6 F5",
        "E7 R4 C7 E4",
        "C3 R5 E2 C4",
        "X7 E5 X3 C5",
        "C2 X4 X1 B6",
        "X5 B7 C0 X2",
        "B5 B3 B1 B2",
        "B4",
    ),
)
SENDS = ((1, 6, 2, 4, 7, 3, 5), (6, 1, 4, 3, 5, 7, 2))


def plan(n):
    if n == 8:
        steps = [[(step[0], int(step[1:])) for step in " ".join(role).split()] for role in ROLES]
        return SENDS, steps
    order = [("R", 0)] + [(op, i) for i in range(1, n) for op in "FR"]
    late = list(range(n - 1, -1, -1))
    order += [(op, i) for i in late for op in "EC"]
    order += [(op, i) for op in "XB" for i in late if i]
    return [list(range(1, n))] * 2, [order] * 2


def layer(
    n, tp, cap,
    q_hbm, k_hbm, v_hbm, sink_hbm, gain_hbm, ids_hbm, rw_hbm,
    ow_hbm, stream_hbm, gate_hbm, up_hbm, down_hbm,
    out_hbm,
    q_ref, k_ref, v_ref, sink_ref, gain_ref, ids_ref, rw_ref,
    ow, stream, gate, up, down,
    halo, own_o, own_m, head, part, part_in, part_sum, part_y, squares,
    pick, mixer, rows_out, slots, scale_out, scale_in, xb, hid,
    po, po_in, chip_sum, sum_y, final, back, mixed, residual, out,
    load_sem, halo_send, halo_recv, ps_send, ps_recv, py_send, py_recv, sq_send, sq_recv,
    d_send, x_recv, sc_send, sc_recv, fc_send, fy_send, f2_send,
    po_send, po_recv, y_send, y_recv, r_send, r_recv, out_sem,
):
    s, t = lax.axis_index("sp"), lax.axis_index("tp")
    ny = tp // CORES
    y, c = t // CORES, lax.rem(t, CORES)
    other = 1 - c
    tok, width = residual.shape
    hidden = gate.shape[1]
    top = ids_ref.shape[0]
    kv_heads = k_ref.shape[0] // HD

    def at_sp(i):
        return (i, t)

    def at_tp(j):
        return (s, j)

    partner = at_tp(y * CORES + other)

    def pair(i):
        total, bit = 0, 1
        while bit < n:
            total = total + lax.rem(s // bit + i // bit, 2) * bit
            bit *= 2
        return total

    def peer_y(dy):
        return lax.rem(y + dy, ny)

    def from_y(dy):
        return lax.rem(y + ny - dy, ny)

    own_cols = pl.ds(pl.multiple_of(t * width, 128), width)
    loads = [
        pltpu.make_async_copy(src, dst, load_sem.at[i])
        for i, (src, dst) in enumerate((
            (k_hbm, k_ref), (v_hbm, v_ref), (q_hbm, q_ref), (ids_hbm, ids_ref),
            (sink_hbm, sink_ref), (rw_hbm, rw_ref), (gain_hbm, gain_ref),
            (ow_hbm, ow), (stream_hbm.at[:, own_cols], stream),
            (gate_hbm.at[0], gate), (up_hbm.at[0], up), (down_hbm.at[0], down),
        ))
    ]
    for load in loads[:7]:
        load.start()

    barrier = pltpu.get_barrier_semaphore()

    def greet_sp(i, _):
        pl.semaphore_signal(
            barrier, inc=1, device_id=at_sp(lax.rem(s + i, n)), device_id_type=MESH
        )
        return 0

    def greet_tp(j, _):
        pl.semaphore_signal(
            barrier, inc=1, device_id=at_tp(lax.rem(t + j, tp)), device_id_type=MESH
        )
        return 0

    lax.fori_loop(1, n, greet_sp, 0)
    lax.fori_loop(1, tp, greet_tp, 0)
    loads[0].wait()
    loads[1].wait()
    loads[3].wait()
    for load in loads[7:9]:
        load.start()
    with scope("barrier"):
        pl.semaphore_wait(barrier, n - 1 + tp - 1)

    right, left = at_sp(lax.rem(s + 1, n)), at_sp(lax.rem(s + n - 1, n))
    last = tok - WINDOW

    def send_right():
        @pl.when(s < n - 1)
        def _():
            for a, source in enumerate((k_ref, v_ref)):
                send(source.at[:, pl.ds(last, WINDOW)], halo.at[0, a],
                     halo_send.at[0], halo_recv.at[0, a], right)

    def send_left():
        @pl.when(s > 0)
        def _():
            for a, source in enumerate((k_ref, v_ref)):
                send(source.at[:, pl.ds(0, WINDOW)], halo.at[1, a],
                     halo_send.at[1], halo_recv.at[1, a], left)

    even = lax.rem(s, 2) == 0
    odd = jnp.logical_not(even)
    pl.when(even)(send_right)
    pl.when(odd)(send_left)
    for load in loads[9:]:
        load.start()

    @pl.when(s == 0)
    def _():
        halo[0] = jnp.zeros(halo.shape[1:], BF16)

    @pl.when(s == n - 1)
    def _():
        halo[1] = jnp.zeros(halo.shape[1:], BF16)

    loads[2].wait()
    loads[4].wait()
    square = (WINDOW, WINDOW)
    ahead = iota(square, 1) - iota(square, 0)
    low_lanes = iota(square, 1) < HD

    def query(b, g):
        rows = pl.ds(pl.multiple_of(b * WINDOW, WINDOW), WINDOW)
        return q_ref[rows, pl.ds(g * 2 * HD, 2 * HD)] * (1.0 / math.sqrt(HD))

    def mix_matrix(v):
        return jnp.concatenate([diagonal(v), diagonal(jnp.ones(v.shape, BF16))], axis=0)

    def sinks(g):
        return [sink_ref[0:1, 2 * g + h : 2 * g + h + 1] for h in range(2)]

    with scope("attn_own"):
        for g in range(kv_heads):
            feats = pl.ds(g * HD, HD)
            keys = diagonal(k_ref[feats, :])
            mixer_v = mix_matrix(v_ref[feats, :])
            for b in range(BLOCKS):
                scores = dot(query(b, g), keys)
                weights = []
                for h in range(2):
                    part_s = [
                        scores[:, h * tok + kb * WINDOW : h * tok + (kb + 1) * WINDOW]
                        for kb in range(BLOCKS)
                    ]
                    if b == 0:
                        part_s[1] = jnp.where(ahead <= 0, part_s[1], MASKED)
                    else:
                        part_s[0] = jnp.where(ahead >= 0, part_s[0], MASKED)
                    row_top = jnp.max(
                        jnp.maximum(part_s[0], part_s[1]), axis=1, keepdims=True
                    )
                    row_top = jnp.maximum(row_top, sinks(g)[h])
                    own_m[b, g, h] = jnp.broadcast_to(row_top, square)
                    weights += [jnp.exp(p - row_top).astype(BF16) for p in part_s]
                own_o[b, g] = dot_t(jnp.concatenate(weights, axis=1), mixer_v)

    with scope("routing"):
        lanes = iota((tok, 128), 1).astype(F32)
        before = (iota((tok, tok), 1) < iota((tok, tok), 0)).astype(BF16)

        ids = [as_column(ids_ref[k : k + 1, :].astype(F32)) for k in range(top)]
        hits = [(lanes == ids[k]).astype(F32) for k in range(top)]
        earlier = dot(before, functools.reduce(jnp.add, hits).astype(BF16))
        place = [
            jnp.sum(earlier * hits[k], axis=1, keepdims=True) + ids[k] * cap
            for k in range(top)
        ]
        place_row = [as_row(p) for p in place]
        loads[5].wait()
        share = [as_column(rw_ref[k : k + 1, :]) for k in range(top)]

        def picks(i, _):
            base = pair(i) * cap
            wanted = (iota((cap, tok), 0) + base).astype(F32)
            hit = functools.reduce(jnp.logical_or, [wanted == p for p in place_row])
            pick[pl.ds(pl.multiple_of(i * cap, cap), cap), :] = hit.astype(F32).astype(BF16)
            spot = (iota((tok, cap), 1) + base).astype(F32)
            weight = functools.reduce(
                jnp.add, [jnp.where(spot == p, w, 0.0) for p, w in zip(place, share)]
            )
            high = weight.astype(BF16)
            mixer[i] = jnp.concatenate([high, (weight - high.astype(F32)).astype(BF16)], axis=1)
            return 0

        lax.fori_loop(0, n, picks, 0)
    pl.when(even)(send_left)
    pl.when(odd)(send_right)
    loads[6].wait()
    loads[7].wait()
    loads[8].wait()
    gain = gain_ref[:, own_cols]

    def attend(b):
        side = 1 - 2 * b
        edge = s + b * n
        inside = jnp.logical_and(edge > 0, edge < 2 * n - 1)

        def arrived(a):
            @pl.when(inside)
            def _():
                landed(halo.at[b, a], halo_recv.at[b, a], left)

        visible = (ahead * side >= 0) & (jnp.broadcast_to(inside.astype(jnp.int32), square) > 0)
        rows = pl.ds(pl.multiple_of(b * WINDOW, WINDOW), WINDOW)
        arrived(0)
        held = []
        for g in range(kv_heads):
            feats = pl.ds(g * HD, HD)
            scores = dot(query(b, g), diagonal(halo[b, 0, feats, :]))
            weights, gap, rest = [], [], []
            for h in range(2):
                piece = jnp.where(visible, scores[:, h * WINDOW : (h + 1) * WINDOW], MASKED)
                before_top = own_m[b, g, h]
                row_top = jnp.max(jnp.maximum(piece, before_top), axis=1, keepdims=True)
                weights.append(jnp.exp(piece - row_top).astype(BF16))
                gap.append(before_top - row_top)
                rest.append(jnp.broadcast_to(sinks(g)[h] - row_top, square))
            shrink = jnp.exp(jnp.where(low_lanes, gap[0], gap[1]))
            total = jnp.exp(jnp.where(low_lanes, rest[0], rest[1]))
            held.append((jnp.concatenate(weights, axis=1), shrink, total))
        arrived(1)
        for g, (weights, shrink, total) in enumerate(held):
            feats = pl.ds(g * HD, HD)
            added = dot_t(weights, mix_matrix(halo[b, 1, feats, :]))
            old = own_o[b, g]
            total = total + old[:, 2 * HD :] * shrink + added[:, 2 * HD :]
            value = old[:, : 2 * HD] * shrink + added[:, : 2 * HD]
            head[rows, pl.ds(g * 2 * HD, 2 * HD)] = (value / total).astype(BF16)

    def project(b, core, yy):
        mine = head[pl.ds(pl.multiple_of(b * WINDOW, WINDOW), WINDOW), :]
        start = pl.multiple_of((yy * CORES + core) * width, 128)
        part[b, core, yy] = dot(mine, ow[:, pl.ds(start, width)]).astype(BF16)

    def swap(b):
        for dy in list(range(1, ny)) + [0]:
            yy = peer_y(dy)
            project(b, other, yy)
            send(part.at[b, other, yy], part_in.at[b, yy], ps_send, ps_recv.at[b, yy], partner)
            project(b, c, yy)

    def across(b):
        for dy in range(1, ny):
            yy = peer_y(dy)
            landed(part_in.at[b, yy], ps_recv.at[b, yy], partner)
            part_sum[b, dy] = (
                part[b, c, yy].astype(F32) + part_in[b, yy].astype(F32)
            ).astype(BF16)
            send(part_sum.at[b, dy], part_y.at[b, dy], py_send, py_recv.at[b, dy - 1],
                 at_tp(yy * CORES + c))

    def settle(b):
        landed(part_in.at[b, y], ps_recv.at[b, y], partner)
        attn = part[b, c, y].astype(F32) + part_in[b, y].astype(F32)
        for dy in range(1, ny):
            landed(part_y.at[b, dy], py_recv.at[b, dy - 1], at_tp(from_y(dy) * CORES + c))
            attn = attn + part_y[b, dy].astype(F32)
        rows = pl.ds(pl.multiple_of(b * WINDOW, WINDOW), WINDOW)
        res = (stream[rows, :].astype(F32) + attn.astype(BF16).astype(F32)).astype(BF16)
        residual[rows, :] = res
        res = res.astype(F32)
        rows_out[rows, :] = (res * gain).astype(BF16)
        squares[0, :, rows] = jnp.broadcast_to(
            as_row(jnp.sum(res * res, axis=1, keepdims=True)), (8, WINDOW)
        )

    first = 1 - lax.rem(s, 2)
    second = 1 - first
    with scope("attend0"):
        attend(first)
    with scope("swap0"):
        swap(first)
    with scope("across0"):
        across(first)
    with scope("attend1"):
        attend(second)
    with scope("swap1"):
        swap(second)
    with scope("across1"):
        across(second)
    with scope("settle0"):
        settle(first)
    with scope("settle1"):
        settle(second)
    for dt in range(1, tp):
        send(squares.at[0], squares.at[dt], sq_send, sq_recv.at[dt - 1],
             at_tp(lax.rem(t + dt, tp)))

    sends, steps = plan(n)
    place_z = s // CHIPS_X
    outer = (place_z == 0) | (place_z == n // CHIPS_X - 1)

    def packed(tables):
        tables = [table + [0] * (-len(table) % DIGITS) for table in map(list, tables)]
        words = [
            [sum(d * BASE**p for p, d in enumerate(table[at : at + DIGITS]))
             for at in range(0, len(table), DIGITS)]
            for table in tables
        ]
        return [jnp.where(outer, b, a) for a, b in zip(*words)]

    def unpacked(k, words):
        word = choose(k // DIGITS, words)
        return choose(k % DIGITS, [word // BASE**p % BASE for p in range(DIGITS)])

    send_words = packed(sends)
    early = jnp.where(outer, EARLY[1], EARLY[0])


    def chosen(i, source):
        rows = pick[pl.ds(pl.multiple_of(i * cap, cap), cap), :]
        return dot(rows, source[...]).astype(BF16)

    def forward(i):
        @pl.when(i > 0)
        def _():
            landed(xb.at[t, i], x_recv.at[t, i], right)

        for dy in range(1, ny):
            send(xb.at[t, i], xb.at[t, i], fy_send, x_recv.at[t, i],
                 at_tp(peer_y(dy) * CORES + c))
        send(xb.at[t, i], xb.at[t, i], fc_send, x_recv.at[t, i], partner)

    def dispatch(k, _):
        i = unpacked(k, send_words)
        slots[i] = chosen(i, rows_out)
        send(slots.at[i], xb.at[t, i], d_send, x_recv.at[t, i], at_sp(pair(i)))
        return 0

    with scope("dispatch"):
        xb[t, 0] = chosen(0, rows_out)
        forward(0)
        lax.fori_loop(0, early, dispatch, 0)

    with scope("scales"):
        square_sum = squares[0]
        for dt in range(1, tp):
            landed(squares.at[dt], sq_recv.at[dt - 1], at_tp(lax.rem(t + tp - dt, tp)))
            square_sum = square_sum + squares[dt]
        inverse = lax.rsqrt(square_sum / (tp * width) + EPSILON)
        high = inverse.astype(BF16).astype(F32)
        middle = (inverse - high).astype(BF16).astype(F32)
        low = inverse - high - middle
        level = iota(inverse.shape, 0)
        pieces = jnp.where(
            level == 0, high, jnp.where(level == 1, middle, jnp.where(level == 2, low, 0.0))
        ).astype(BF16)
        scales = jnp.sum(dot_t(pieces, pick[...]), axis=0, keepdims=True)
        for i in range(n):
            piece = jnp.broadcast_to(scales[:, i * cap : (i + 1) * cap], (8, cap))
            if i == 0:
                scale_in[0] = piece
            else:
                scale_out[i] = piece
                send(scale_out.at[i], scale_in.at[i], sc_send, sc_recv.at[i],
                     at_sp(pair(i)))

    with scope("late"):
        lax.fori_loop(early, n - 1, dispatch, 0)

    with scope("weights"):
        for load in loads[9:]:
            load.wait()

    def relay(i):
        for dy in range(1, ny):
            j = from_y(dy) * CORES + c
            landed(xb.at[j, i], x_recv.at[j, i], at_tp(j))
            send(xb.at[j, i], xb.at[j, i], f2_send, x_recv.at[j, i], partner)

    tile = min(hidden, 256)

    def expert(i):
        for yy in range(ny):
            j = yy * CORES + other
            landed(xb.at[j, i], x_recv.at[j, i], partner)

        @pl.when(i > 0)
        def _():
            landed(scale_in.at[i], sc_recv.at[i], right)

        scale = as_column(scale_in[i, 0:1, :])
        rows = jnp.concatenate([xb[j, i] for j in range(tp)], axis=1)
        for f in range(hidden // tile):
            cols = pl.ds(f * tile, tile)
            gate_pre = dot(rows, gate[:, cols]) * scale
            upward = dot(rows, up[:, cols]) * scale
            hid[:, cols] = (gate_pre / (1.0 + jnp.exp(-gate_pre)) * upward).astype(BF16)
        activated = hid[...]

        def lower(core):
            for yy in range(ny):
                start = pl.multiple_of((yy * CORES + core) * width, 128)
                po[i, core, yy] = dot(activated, down[:, pl.ds(start, width)]).astype(BF16)

        lower(other)
        send(po.at[i, other], po_in.at[i], po_send, po_recv.at[i], partner)
        lower(c)

    def chip_add(i):
        landed(po_in.at[i], po_recv.at[i], partner)
        for dy in range(1, ny):
            yy = peer_y(dy)
            chip_sum[dy, i] = (po[i, c, yy].astype(F32) + po_in[i, yy].astype(F32)).astype(BF16)
            send(chip_sum.at[dy, i], sum_y.at[dy, i], y_send, y_recv.at[dy - 1, i],
                 at_tp(yy * CORES + c))

    def whole(i):
        total = po[i, c, y].astype(F32) + po_in[i, y].astype(F32)
        for dy in range(1, ny):
            landed(sum_y.at[dy, i], y_recv.at[dy - 1, i], at_tp(from_y(dy) * CORES + c))
            total = total + sum_y[dy, i].astype(F32)
        return total.astype(BF16)

    def finish(i):
        final[i] = whole(i)
        send(final.at[i], back.at[i], r_send, r_recv.at[i], at_sp(pair(i)))

    def blend(i):
        rows = back[i]
        return dot(mixer[i], jnp.concatenate([rows, rows], axis=0))

    def returned(i):
        landed(back.at[i], r_recv.at[i], right)
        mixed[...] += blend(i)

    mixed[...] = residual[...].astype(F32)
    stages = dict(
        F=forward, R=relay, E=expert, C=chip_add, X=finish, B=returned
    )
    codes = [
        [list(stages).index(op) * n + i for op, i in order] for order in steps
    ]

    code_words = packed(codes)

    def step(k, _):
        code = unpacked(k, code_words)
        for at, (name, stage) in enumerate(stages.items()):
            @pl.when((code >= at * n) & (code < (at + 1) * n))
            def _(stage=stage, name=name, at=at):
                with scope(name):
                    stage(code - at * n)
        return 0

    lax.fori_loop(0, len(codes[0]), step, 0)

    with scope("drain"):
        @pl.when(s < n - 1)
        def _():
            sent(halo.at[0], halo_send.at[0], right)

        @pl.when(s > 0)
        def _():
            sent(halo.at[1], halo_send.at[1], left)

        others = pl.ds(1, ny - 1)
        sent(part_in, ps_send, partner)
        sent(part_sum.at[:, others], py_send, partner)
        sent(squares.at[pl.ds(1, tp - 1)], sq_send, partner)
        sent(slots.at[pl.ds(1, n - 1)], d_send, right)
        sent(scale_out.at[pl.ds(1, n - 1)], sc_send, right)
        sent(final, fc_send, partner)
        sent(po_in, po_send, partner)
        for sem in (fy_send, f2_send):
            sent(chip_sum.at[others], sem, partner)

    with scope("own"):
        back[0] = whole(0)
        out[...] = (mixed[...] + blend(0)).astype(BF16)
    put = pltpu.make_async_copy(out, out_hbm, out_sem)
    put.start()
    sent(chip_sum.at[others], y_send, partner)
    sent(final.at[pl.ds(1, n - 1)], r_send, right)
    put.wait()


def local(
    n, tp,
    queries, key_columns, value_columns, sink_logits, out_weight, stream_in, norm_gain,
    expert_ids, route_weights, gate_weight, up_weight, down_weight,
):
    tok, features = stream_in.shape
    ny = tp // CORES
    cap = 4 * tok // n
    width = features // tp
    hidden = gate_weight.shape[2]
    kv = key_columns.shape[0]
    top = expert_ids.shape[1]
    heads = sink_logits.shape[0]
    groups = kv // HD
    assert tok == BLOCKS * WINDOW and heads == 2 * groups
    dma = pltpu.SemaphoreType.DMA
    anywhere = pl.BlockSpec(memory_space=pl.ANY)
    scratch = [
        pltpu.VMEM(queries.shape, BF16),
        pltpu.VMEM(key_columns.shape, BF16),
        pltpu.VMEM(value_columns.shape, BF16),
        pltpu.VMEM((1, heads), F32),
        pltpu.VMEM((1, features), F32),
        pltpu.VMEM((top, tok), jnp.int32),
        pltpu.VMEM((top, tok), F32),
        pltpu.VMEM(out_weight.shape, BF16),
        pltpu.VMEM((tok, width), BF16),
        pltpu.VMEM(gate_weight.shape[1:], BF16),
        pltpu.VMEM(up_weight.shape[1:], BF16),
        pltpu.VMEM(down_weight.shape[1:], BF16),
        pltpu.VMEM((2, 2, kv, WINDOW), BF16),
        pltpu.VMEM((BLOCKS, groups, WINDOW, 4 * HD), F32),
        pltpu.VMEM((BLOCKS, groups, 2, WINDOW, WINDOW), F32),
        pltpu.VMEM(queries.shape, BF16),
        pltpu.VMEM((BLOCKS, CORES, ny, WINDOW, width), BF16),
        pltpu.VMEM((BLOCKS, ny, WINDOW, width), BF16),
        pltpu.VMEM((BLOCKS, ny, WINDOW, width), BF16),
        pltpu.VMEM((BLOCKS, ny, WINDOW, width), BF16),
        pltpu.VMEM((tp, 8, tok), F32),
        pltpu.VMEM((n * cap, tok), BF16),
        pltpu.VMEM((n, tok, 2 * cap), BF16),
        pltpu.VMEM((tok, width), BF16),
        pltpu.VMEM((n, cap, width), BF16),
        pltpu.VMEM((n, 8, cap), F32),
        pltpu.VMEM((n, 8, cap), F32),
        pltpu.VMEM((tp, n, cap, width), BF16),
        pltpu.VMEM((cap, hidden), BF16),
        pltpu.VMEM((n, CORES, ny, cap, width), BF16),
        pltpu.VMEM((n, ny, cap, width), BF16),
        pltpu.VMEM((ny, n, cap, width), BF16),
        pltpu.VMEM((ny, n, cap, width), BF16),
        pltpu.VMEM((n, cap, width), BF16),
        pltpu.VMEM((n, cap, width), BF16),
        pltpu.VMEM((tok, width), F32),
        pltpu.VMEM((tok, width), BF16),
        pltpu.VMEM((tok, width), BF16),
        dma((12,)),
        dma((2,)), dma((2, 2)),
        dma, dma((BLOCKS, ny)),
        dma, dma((BLOCKS, ny - 1)),
        dma, dma((tp - 1,)),
        dma, dma((tp, n)), dma, dma((n,)),
        dma, dma, dma,
        dma, dma((n,)),
        dma, dma((ny - 1, n)),
        dma, dma((n,)),
        dma,
    ]
    return pl.pallas_call(
        functools.partial(layer, n, tp, cap),
        out_shape=jax.ShapeDtypeStruct((tok, width), BF16),
        in_specs=[anywhere] * 12,
        out_specs=anywhere,
        scratch_shapes=scratch,
        compiler_params=pltpu.CompilerParams(
            collective_id=0, has_side_effects=True, vmem_limit_bytes=60 * 1024 * 1024
        ),
    )(
        queries, key_columns, value_columns, sink_logits[None, :], norm_gain[None, :],
        expert_ids.T, route_weights.T, out_weight, stream_in, gate_weight, up_weight,
        down_weight,
    )


def solution(mesh):
    placed = (
        P("sp", "tp"),
        P("tp", "sp"),
        P("tp", "sp"),
        P("tp"),
        P("tp", None),
        P("sp", None),
        P(),
        P("sp", None),
        P("sp", None),
        P("sp", None, "tp"),
        P("sp", None, "tp"),
        P("sp", "tp", None),
    )
    return jax.shard_map(
        functools.partial(local, mesh.shape["sp"], mesh.shape["tp"]),
        mesh=mesh, in_specs=placed, out_specs=P("sp", "tp"), check_vma=False,
    )
```
